32 devices in a mesh: sp: 4 (over z), fs: 4 (over y, x), tp: 2 (over core).
Axes of the slice: x: 2, y: 2, z: 4, core: 2. Of those that a mesh axis runs over, the one named last changes fastest.
Arguments:
- tokens: bfloat16 [4, 2048, 2048], P('fs', ('sp', 'tp')), may hold values from -6 to 6
- norm_gain: float32 [2048], replicated, may hold values from 0.1 to 1.9
- query_weight: bfloat16 [2048, 1024], P('sp', 'tp'), may hold values from -20 to 20
- key_matrix: bfloat16 [2048, 256], P('sp', 'tp'), may hold values from -0.125 to 0.125
- value_matrix: bfloat16 [2048, 256], P('sp', 'tp'), may hold values from -0.125 to 0.125
- pool_in_weight: bfloat16 [2048, 1024], P('sp', 'tp'), may hold values from -0.125 to 0.125
- head_sink_logit: float32 [16], replicated, may hold values from 2 to 6
- pool_mix: bfloat16 [4, 256, 256], replicated, may hold values from -0.375 to 0.375
- pool_gain: float32 [1024], replicated, may hold values from 0.1 to 1.9
- attn_out_weight: bfloat16 [1024, 2048], P('tp', 'sp'), may hold values from -1 to 1
- pool_out_weight: bfloat16 [1024, 2048], P('tp', 'sp'), may hold values from -0.125 to 0.125
Outputs:
- mixed: bfloat16 [4, 2048, 2048], P('fs', ('sp', 'tp'))
- row_log_weight_sum: float32 [4, 16, 2048], P('fs', 'tp', 'sp')
The draws below stay inside these ranges and needn't reach their ends.
All inputs are finite; a program needn't handle non-finite values.
Results may differ from the reference program's by a relative error of at most 0.0095.
The reference program's roundings to bfloat16 on the way count: a program that leaves them out, or rounds other values in their place, can miss the bound.
Values may be sent and summed in bfloat16 or wider, within the bound.
A program may use at most 64 MiB of HBM per device.

```python
import jax
import jax.numpy as jnp
from jax import lax

MODEL_WIDTH = 2048
HEAD_SIZE = 64
QUERY_HEADS = 16
KEY_VALUE_HEADS = 4
WINDOW = 128
POOL_GROUPS = 4
POOL_CH = 256
LEN = 2048
SEQS = 4


def draw_query_weight(key, part):
    base = jax.random.normal(jax.random.fold_in(key, 11), (MODEL_WIDTH, QUERY_HEADS * HEAD_SIZE), jnp.float32)
    base = jnp.clip(base, -6.0, 6.0) * MODEL_WIDTH ** (-0.5)
    return jnp.clip(base, -20.0, 20.0).astype(jnp.bfloat16)


def levels(rng, shape, shards, least, high):
    def one(axis_at, parts):
        heights = jax.random.uniform(jax.random.fold_in(jax.random.fold_in(rng, 6), axis_at), (parts,), jnp.float32, least / len(shards), high / len(shards))
        return jnp.repeat(jnp.exp(heights), shape[axis_at] // parts).reshape((-1,) + (1,) * (len(shape) - axis_at - 1))

    level = one(*shards[0])
    for cut in shards[1:]:
        level = level * one(*cut)
    return level


def bell_draw(rng, extent, deviation, reach, cuts=(), kind=jnp.bfloat16):
    values = deviation * jax.random.normal(rng, extent, jnp.float32)
    if cuts:
        values = values * levels(rng, extent, cuts, -0.22, 0.18)
    return jnp.clip(values, -reach, reach).astype(kind)


def setup_inputs(seed: int = 0) -> dict:
    seeds = jax.random.split(jax.random.key(seed), 12)
    return {
        "tokens": bell_draw(seeds[0], (SEQS, LEN, MODEL_WIDTH), 1.0, 6.0, ((0, 4), (1, 8))),
        "norm_gain": jnp.clip(1.0 + 0.18 * jax.random.normal(seeds[1], (MODEL_WIDTH,), jnp.float32), 0.1, 1.9),
        "query_weight": draw_query_weight(jax.random.fold_in(seeds[11], 71), 0),
        "key_matrix": bell_draw(seeds[3], (MODEL_WIDTH, KEY_VALUE_HEADS * HEAD_SIZE), MODEL_WIDTH ** -0.5, 0.125, ((0, 4), (1, 2))),
        "value_matrix": bell_draw(seeds[4], (MODEL_WIDTH, KEY_VALUE_HEADS * HEAD_SIZE), MODEL_WIDTH ** -0.5, 0.125, ((0, 4), (1, 2))),
        "pool_in_weight": bell_draw(seeds[5], (MODEL_WIDTH, POOL_GROUPS * POOL_CH), MODEL_WIDTH ** -0.5, 0.125, ((0, 4), (1, 2))),
        "head_sink_logit": jnp.clip(jax.random.uniform(seeds[6], (QUERY_HEADS,), jnp.float32, 2.0, 6.0), 2.0, 6.0),
        "pool_mix": bell_draw(seeds[7], (POOL_GROUPS, POOL_CH, POOL_CH), POOL_CH ** -0.5, 0.375),
        "pool_gain": jnp.clip(1.0 + 0.18 * jax.random.normal(seeds[8], (POOL_GROUPS * POOL_CH,), jnp.float32), 0.1, 1.9),
        "attn_out_weight": bell_draw(seeds[9], (QUERY_HEADS * HEAD_SIZE, MODEL_WIDTH), (QUERY_HEADS * HEAD_SIZE // 32) ** -0.5, 1.0, ((0, 2), (1, 4))),
        "pool_out_weight": bell_draw(seeds[10], (POOL_GROUPS * POOL_CH, MODEL_WIDTH), (QUERY_HEADS * HEAD_SIZE + POOL_GROUPS * POOL_CH) ** -0.5, 0.125, ((0, 2), (1, 4))),
    }


EPSILON = 1e-06
POOL_SPANS = (2, 4, 8, 16)

def windowed_attend(query_rows, key_rows, value_rows, sinks, kv_heads, group):
    rows = query_rows.shape[0]
    blocks = rows // WINDOW
    width = key_rows.shape[1]
    ext_keys = jnp.concatenate([jnp.zeros((WINDOW, width), key_rows.dtype), key_rows], 0)
    ext_values = jnp.concatenate([jnp.zeros((WINDOW, width), value_rows.dtype), value_rows], 0)

    def banded(table):
        return jnp.concatenate([table[:rows].reshape(blocks, WINDOW, width), table[WINDOW:].reshape(blocks, WINDOW, width)], axis=1)
    band_keys = banded(ext_keys).reshape(blocks, 2 * WINDOW, kv_heads, HEAD_SIZE).astype(jnp.float32)
    band_values = banded(ext_values).reshape(blocks, 2 * WINDOW, kv_heads, HEAD_SIZE).astype(jnp.float32)
    query_blocks = query_rows.reshape(blocks, WINDOW, kv_heads, group, HEAD_SIZE).astype(jnp.float32)
    scores = jnp.einsum('bqkgd,bskd->bkgqs', query_blocks, band_keys) * HEAD_SIZE ** (-0.5)
    query_pos = jnp.arange(rows).reshape(blocks, WINDOW, 1)
    key_pos = jnp.arange(blocks).reshape(blocks, 1, 1) * WINDOW - WINDOW + jnp.arange(2 * WINDOW).reshape(1, 1, 2 * WINDOW)
    offset = query_pos - key_pos
    allowed = (offset >= 0) & (offset < WINDOW) & (key_pos >= 0)
    scores = jnp.where(allowed[:, None, None], scores, -jnp.inf)
    sink_grid = sinks.astype(jnp.float32).reshape(1, kv_heads, group, 1, 1)
    top = jnp.maximum(lax.optimization_barrier(jnp.max(scores, axis=-1, keepdims=True)), sink_grid)
    weights = jnp.exp(scores - top)
    total = lax.optimization_barrier(jnp.sum(weights, axis=-1, keepdims=True)) + jnp.exp(sink_grid - top)
    probs = (weights / total).astype(jnp.bfloat16).astype(jnp.float32)
    mixed = jnp.einsum('bkgqs,bskd->bqkgd', probs, band_values).astype(jnp.bfloat16)
    row_log_weight_sum = (top + jnp.log(total))[..., 0]
    return (mixed.reshape(rows, kv_heads * group * HEAD_SIZE), row_log_weight_sum.transpose(1, 2, 0, 3).reshape(kv_heads * group, rows))

def pool_branch(pool_input, pool_mix, pool_gain):
    rows = pool_input.shape[0]
    pool_reach = max(POOL_SPANS)
    padded = jnp.concatenate([jnp.zeros((pool_reach, pool_input.shape[1]), jnp.float32), pool_input.astype(jnp.float32)], 0)
    position = jnp.arange(rows).reshape(rows, 1)
    pieces = []
    for index, span in enumerate(POOL_SPANS):
        columns = padded[:, index * POOL_CH:(index + 1) * POOL_CH]
        trailing = jnp.zeros((rows, POOL_CH), jnp.float32)
        for lag in range(span):
            trailing = trailing + columns[pool_reach - lag:pool_reach - lag + rows]
        count = jnp.minimum(position + 1, span).astype(jnp.float32)
        pieces.append(trailing / count - columns[pool_reach:])
    centred = jnp.concatenate(pieces, axis=1).astype(jnp.bfloat16)
    grouped = centred.reshape(rows, POOL_GROUPS, POOL_CH).astype(jnp.float32)
    product = jnp.einsum('rgc,gcd->rgd', grouped, pool_mix.astype(jnp.float32)).reshape(rows, POOL_GROUPS * POOL_CH)
    return (product * pool_gain).astype(jnp.bfloat16)

def reference(tokens, norm_gain, query_weight, key_matrix, value_matrix, pool_in_weight, head_sink_logit, pool_mix, pool_gain, attn_out_weight, pool_out_weight):

    def one_sequence(sequence):
        values_f = sequence.astype(jnp.float32)
        scale = lax.rsqrt(lax.optimization_barrier(jnp.mean(values_f * values_f, axis=-1, keepdims=True)) + EPSILON)
        normed = (values_f * scale * norm_gain).astype(jnp.bfloat16)
        query_rows = jnp.dot(normed, query_weight, preferred_element_type=jnp.float32).astype(jnp.bfloat16)
        key_rows = jnp.dot(normed, key_matrix, preferred_element_type=jnp.float32).astype(jnp.bfloat16)
        value_rows = jnp.dot(normed, value_matrix, preferred_element_type=jnp.float32).astype(jnp.bfloat16)
        pool_input = jnp.dot(normed, pool_in_weight, preferred_element_type=jnp.float32).astype(jnp.bfloat16)
        attention_mixer, row_log_weight_sum = windowed_attend(query_rows, key_rows, value_rows, head_sink_logit, KEY_VALUE_HEADS, QUERY_HEADS // KEY_VALUE_HEADS)
        pool_out = pool_branch(pool_input, pool_mix, pool_gain)
        result = jnp.dot(attention_mixer, attn_out_weight, preferred_element_type=jnp.float32) + jnp.dot(pool_out, pool_out_weight, preferred_element_type=jnp.float32)
        return (result.astype(jnp.bfloat16), row_log_weight_sum)
    mixed, row_log_weight_sum = lax.map(one_sequence, tokens)
    return (mixed, row_log_weight_sum)
```

```python
import functools

import jax
import jax.numpy as jnp
from jax import lax
from jax.experimental import pallas as pl
from jax.experimental.pallas import tpu as pltpu
from jax.sharding import PartitionSpec as P

HEAD_SIZE = 64
WINDOW = 128
POOL_CH = 256


EPSILON = 1e-06
POOL_SPANS = (2, 4, 8, 16)


def passed_along(shard, axis, by):
    size = lax.axis_size(axis)
    pairs = [(i, i + by) for i in range(size) if 0 <= i + by < size]
    return lax.ppermute(shard, axis, pairs)


def windowed_attend(
    query_rows, key_rows, value_rows, key_tail, value_tail, sinks, kv_heads, group, first_pos
):
    rows = query_rows.shape[0]
    blocks = rows // WINDOW
    width = key_rows.shape[1]
    ext_keys = jnp.concatenate([key_tail, key_rows], 0)
    ext_values = jnp.concatenate([value_tail, value_rows], 0)

    def banded(table):
        return jnp.concatenate(
            [
                table[:rows].reshape(blocks, WINDOW, width),
                table[WINDOW:].reshape(blocks, WINDOW, width),
            ],
            axis=1,
        )

    band_keys = banded(ext_keys).reshape(blocks, 2 * WINDOW, kv_heads, HEAD_SIZE)
    band_values = banded(ext_values).reshape(blocks, 2 * WINDOW, kv_heads, HEAD_SIZE)
    query_blocks = query_rows.reshape(blocks, WINDOW, kv_heads, group, HEAD_SIZE)
    scores = jnp.einsum(
        "bqkgd,bskd->bkgqs", query_blocks, band_keys, preferred_element_type=jnp.float32
    ) * HEAD_SIZE ** (-0.5)
    query_pos = first_pos + jnp.arange(rows).reshape(blocks, WINDOW, 1)
    key_pos = (
        first_pos
        - WINDOW
        + jnp.arange(blocks).reshape(blocks, 1, 1) * WINDOW
        + jnp.arange(2 * WINDOW).reshape(1, 1, 2 * WINDOW)
    )
    offset = query_pos - key_pos
    allowed = (offset >= 0) & (offset < WINDOW) & (key_pos >= 0)
    scores = jnp.where(allowed[:, None, None], scores, -jnp.inf)
    sink_grid = sinks.reshape(1, kv_heads, group, 1, 1)
    top = jnp.maximum(jnp.max(scores, axis=-1, keepdims=True), sink_grid)
    weights = jnp.exp(scores - top)
    total = jnp.sum(weights, axis=-1, keepdims=True) + jnp.exp(sink_grid - top)
    probs = (weights / total).astype(jnp.bfloat16)
    mixed = jnp.einsum(
        "bkgqs,bskd->bqkgd", probs, band_values, preferred_element_type=jnp.float32
    ).astype(jnp.bfloat16)
    row_log_weight_sum = (top + jnp.log(total))[..., 0]
    return (
        mixed.reshape(rows, kv_heads * group * HEAD_SIZE),
        row_log_weight_sum.transpose(1, 2, 0, 3).reshape(kv_heads * group, rows),
    )


def pool_branch(pool_rows, pool_tail, mixing, scales, group_start, first_pos):
    rows = pool_rows.shape[0]
    columns = pool_rows.shape[1]
    pool_reach = max(POOL_SPANS)
    extended = jnp.concatenate([pool_tail, pool_rows], 0).astype(jnp.float32)
    group_index = group_start + jnp.arange(columns) // POOL_CH
    span_table = jnp.array(POOL_SPANS, jnp.int32)
    matches = group_index[:, None] == jnp.arange(len(POOL_SPANS))[None, :]
    span_of_col = jnp.sum(jnp.where(matches, span_table[None, :], 0), axis=1)
    trailing = jnp.zeros((rows, columns), jnp.float32)
    for lag in range(pool_reach):
        trailing = trailing + jnp.where(
            lag < span_of_col[None, :], extended[pool_reach - lag : pool_reach - lag + rows], 0.0
        )
    position = first_pos + jnp.arange(rows)
    count = jnp.minimum(position[:, None] + 1, span_of_col[None, :]).astype(jnp.float32)
    centred = (trailing / count - extended[pool_reach:]).astype(jnp.bfloat16)
    grouped = centred.reshape(rows, columns // POOL_CH, POOL_CH)
    product = jnp.einsum(
        "rgc,gcd->rgd", grouped, mixing, preferred_element_type=jnp.float32
    ).reshape(rows, columns)
    return (product * scales).astype(jnp.bfloat16)


def local(
    tokens,
    norm_gain,
    query_weight,
    key_matrix,
    value_matrix,
    pool_in_weight,
    head_sink_logit,
    pool_mix,
    pool_gain,
    attn_out_weight,
    pool_out_weight,
):
    tp_index = lax.axis_index("tp")
    sp_index = lax.axis_index("sp")
    q_cols = query_weight.shape[1]
    kv_cols = key_matrix.shape[1]
    pool_cols = pool_in_weight.shape[1]
    q_heads = q_cols // HEAD_SIZE
    kv_heads = kv_cols // HEAD_SIZE
    groups_dev = pool_cols // POOL_CH
    full_query, full_key, full_value, full_pool = (
        lax.all_gather(query_weight, "sp", axis=0, tiled=True),
        lax.all_gather(key_matrix, "sp", axis=0, tiled=True),
        lax.all_gather(value_matrix, "sp", axis=0, tiled=True),
        lax.all_gather(pool_in_weight, "sp", axis=0, tiled=True),
    )
    values_f = lax.all_gather(tokens[0], "tp", axis=0, tiled=True).astype(jnp.float32)
    scale = lax.rsqrt(jnp.mean(values_f * values_f, axis=-1, keepdims=True) + EPSILON)
    normed = (values_f * scale * norm_gain).astype(jnp.bfloat16)
    outputs = [
        jnp.dot(normed, weight, preferred_element_type=jnp.float32).astype(jnp.bfloat16)
        for weight in (full_query, full_key, full_value, full_pool)
    ]
    projected = jnp.concatenate(outputs, axis=1)
    rows = projected.shape[0]
    first_pos = sp_index * rows
    query_rows = projected[:, :q_cols]
    key_rows = projected[:, q_cols : q_cols + kv_cols]
    value_rows = projected[:, q_cols + kv_cols : q_cols + 2 * kv_cols]
    pool_rows = projected[:, q_cols + 2 * kv_cols :]
    pool_reach = max(POOL_SPANS)
    sinks = lax.dynamic_slice_in_dim(head_sink_logit, tp_index * q_heads, q_heads, 0)
    mixing = lax.dynamic_slice_in_dim(pool_mix, tp_index * groups_dev, groups_dev, 0)
    scales = lax.dynamic_slice_in_dim(pool_gain, tp_index * pool_cols, pool_cols, 0)
    key_tail, value_tail, pool_tail = passed_along(
        (key_rows[rows - WINDOW :], value_rows[rows - WINDOW :], pool_rows[rows - pool_reach :]),
        "sp",
        1,
    )
    attn_part, log_part = windowed_attend(
        query_rows,
        key_rows,
        value_rows,
        key_tail,
        value_tail,
        sinks,
        kv_heads,
        q_heads // kv_heads,
        first_pos,
    )
    pool_part = pool_branch(pool_rows, pool_tail, mixing, scales, tp_index * groups_dev, first_pos)
    half_attn, half_pool = (
        lax.all_gather(attn_out_weight, "sp", axis=1, tiled=True),
        lax.all_gather(pool_out_weight, "sp", axis=1, tiled=True),
    )
    result = lax.psum_scatter(
        jnp.dot(attn_part, half_attn, preferred_element_type=jnp.float32)
        + jnp.dot(pool_part, half_pool, preferred_element_type=jnp.float32),
        "tp",
        scatter_dimension=0,
        tiled=True,
    ).astype(jnp.bfloat16)
    return (result[None], log_part[None])


LANES = 128
TILE = 16
OUT_CUTS = 4
MESH_ID = pl.DeviceIdType.MESH


def nearest(n, step, me):
    tables = [sorted((j for j in range(n) if j != z), key=lambda j: (abs(j - z), j)) for z in range(n)]
    shard = jnp.int32(tables[0][step])
    for z in range(1, n):
        shard = jnp.where(me == z, tables[z][step], shard)
    return shard


def layer_kernel(
    n,
    sinks,
    tokens,
    gain,
    wq,
    wk,
    wv,
    wp,
    mix,
    pool_gain,
    wao,
    wpo,
    out,
    log_out,
    held,
    wout,
    kv_in,
    tok,
    gain_v,
    pgain_v,
    sink_v,
    out_v,
    log_v,
    acc_q,
    acc_p,
    nrm,
    qb,
    kvb,
    pool_ext,
    mixed,
    mix_own,
    logs,
    logs_got,
    keep_n,
    send_n,
    got_n,
    y_part,
    y_got,
    mine,
    sent,
    got,
    z_send,
    x_send,
    z_recv,
    x_recv,
    load_sem,
    tok_sem,
    tok_send,
    tok_recv,
    ytok_send,
    ytok_recv,
    fwd_send,
    fwd_recv,
    halo_send,
    halo_recv,
    sumn_send,
    sumn_recv,
    sumo_send,
    sumo_recv,
    yp_send,
    yp_recv,
    log_send,
    log_recv,
    out_sem,
):
    me = lax.axis_index("sp")
    f = lax.axis_index("fs")
    c = lax.axis_index("tp")
    f32, bf16 = jnp.float32, jnp.bfloat16
    half, width = tokens.shape
    rows = 2 * half
    depth = wq.shape[0]
    part_rows = depth // 2
    q_cols = wq.shape[1] // 2
    group = q_cols // HEAD_SIZE
    out_cols = wao.shape[1]
    n_in = held.shape[1]
    n_pieces = n_in + OUT_CUTS
    chunk = half // 4
    blocks = rows // WINDOW
    y, x = f // 2, lax.rem(f, 2)
    beside = f + 1 - 2 * x
    across = lax.rem(f + 2, 4)
    up, down = me + 1, me - 1
    has_up, has_down = me < n - 1, me > 0
    inner = has_up & has_down

    def at_cols(ref, i):
        return ref.at[:, pl.ds(pl.multiple_of(y * q_cols + i * LANES, LANES), LANES)]

    y_rows = pl.ds(pl.multiple_of(y * part_rows, part_rows), part_rows)
    pool_index = 2 * c + y
    norm_order = (2, 0, 1, 3)

    def own_chunk(i, side):
        first = (3, 1, 2, 0) if side == 0 else (0, 2, 1, 3)
        return first[i] * chunk

    def own_at(i):
        return pl.multiple_of(jnp.where(c == 0, own_chunk(i, 0), own_chunk(i, 1)), chunk)

    def tok_load(i):
        at = pl.ds(own_at(i), chunk)
        return pltpu.make_async_copy(tokens.at[at], tok.at[at], tok_sem.at[i])

    first_loads = [
        pltpu.make_async_copy(wk, kv_in.at[0], load_sem.at[0]),
        pltpu.make_async_copy(wv, kv_in.at[1], load_sem.at[0]),
    ]
    for i in range(2):
        first_loads.append(pltpu.make_async_copy(at_cols(wq, i), held.at[me, 1 + i], load_sem.at[0]))
    for i in range(2):
        first_loads.append(pltpu.make_async_copy(at_cols(wp, i), held.at[me, 3 + i], load_sem.at[0]))
    late_loads = [
        pltpu.make_async_copy(wao.at[y_rows], wout.at[me, pl.ds(0, part_rows)], load_sem.at[1]),
        pltpu.make_async_copy(wpo.at[y_rows], wout.at[me, pl.ds(part_rows, part_rows)], load_sem.at[2]),
        pltpu.make_async_copy(mix.at[pool_index], mix_own, load_sem.at[3]),
        pltpu.make_async_copy(pool_gain, pgain_v, load_sem.at[4]),
        pltpu.make_async_copy(sinks, sink_v, load_sem.at[5]),
    ]
    gain_load = pltpu.make_async_copy(gain, gain_v, load_sem.at[6])
    for cp in first_loads[:2]:
        cp.start()
    tok_load(norm_order[0]).start()
    gain_load.start()
    for cp in first_loads[2:]:
        cp.start()
    for i in norm_order[1:]:
        tok_load(i).start()
    for cp in late_loads:
        cp.start()

    barrier = pltpu.get_barrier_semaphore()
    for peer in ({"tp": 1 - c}, {"fs": beside}, {"fs": across}, {"fs": across, "tp": 1 - c}):
        pl.semaphore_signal(barrier, inc=1, device_id=peer, device_id_type=MESH_ID)

    @pl.when(has_up)
    def _():
        pl.semaphore_signal(barrier, inc=1, device_id={"sp": up}, device_id_type=MESH_ID)

    @pl.when(has_down)
    def _():
        pl.semaphore_signal(barrier, inc=1, device_id={"sp": down}, device_id_type=MESH_ID)

    def remote(src, dst, send, recv, to):
        return pltpu.make_async_remote_copy(src, dst, send, recv, device_id=to, device_id_type=MESH_ID)

    def piece(s, j, part):
        if s < n_in:
            return held.at[j, s, pl.ds(pl.multiple_of(part * part_rows, part_rows), part_rows)]
        size = part_rows // OUT_CUTS
        return wout.at[j, pl.ds(pl.multiple_of(part * part_rows + (s - n_in) * size, size), size)]

    def bulk(count):
        return nrm.at[0, pl.ds(0, count * part_rows * LANES // width)]

    def sent_all(ref, sem):
        pltpu.make_async_remote_copy(ref, ref, sem, sem, device_id={"tp": 1 - c}, device_id_type=MESH_ID).wait_send()

    def got_all(ref, sem):
        pltpu.make_async_remote_copy(ref, ref, sem, sem, device_id={"tp": 1 - c}, device_id_type=MESH_ID).wait_recv()

    def z_hop(s, j, way):
        block = piece(s, j, x)
        to = me if way is None else jnp.where(way == 0, up, down)
        slot = z_recv.at[s, lax.rem(j - to + n, n) - 1]
        return remote(block, block, z_send.at[0 if way is None else way], slot, {"sp": to})

    def x_group(s, k):
        if s >= n_in:
            return 5 + k
        return 0 if s == 0 else 1 + 2 * ((s - 1) // 2) + k // (n - 2)

    def x_hop(s, k):
        block = piece(s, shard[k], x)
        return remote(block, block, x_send, x_recv.at[x_group(s, k)], {"fs": beside})

    def onward(j):
        return jnp.where(j < me, 0, 1), ((j < me) & has_up) | ((j > me) & has_down)

    def own_send(s):
        @pl.when(has_up)
        def _():
            z_hop(s, me, 0).start()

        @pl.when(has_down)
        def _():
            z_hop(s, me, 1).start()

    shard = [nearest(n, k, me) for k in range(n - 1)]
    def pass_on(s, k):
        j = shard[k]
        z_hop(s, j, None).wait_recv()
        way, more = onward(j)

        @pl.when(more)
        def _():
            z_hop(s, j, way).start()

        x_hop(s, k).start()

    def inner_slot(s, k):
        @pl.when(inner)
        def _():
            pass_on(s, k)

    def end_slot(s, k):
        @pl.when(jnp.logical_not(inner))
        def _():
            pass_on(s, k)

    def send_inner(s):
        @pl.when(inner)
        def _():
            own_send(s)

    def send_end(s):
        @pl.when(jnp.logical_not(inner))
        def _():
            own_send(s)

    def pick(a, b):
        return pl.ds(pl.multiple_of(jnp.where(c == 0, a, b), chunk), chunk)

    def tok_hop(i):
        block = nrm.at[0, pick(own_chunk(i, 0), half + own_chunk(i, 1))]
        return remote(block, block, tok_send, tok_recv, {"tp": 1 - c})

    low_order = (2, 4, 6, 0)
    high_order = (5, 3, 7, 1)

    def y_tok(i):
        where = pick(low_order[i] * chunk, high_order[i] * chunk)
        return remote(nrm.at[0, where], nrm.at[1, where], ytok_send, ytok_recv.at[i], {"fs": across})

    def fwd(i):
        block = nrm.at[1, pick(low_order[i] * chunk, high_order[i] * chunk)]
        return remote(block, block, fwd_send, fwd_recv.at[i], {"tp": 1 - c})

    @pl.when(me == 0)
    def _():
        for s in range(2):
            kvb[s, pl.ds(0, WINDOW), :] = jnp.zeros((WINDOW, kvb.shape[2]), bf16)
            pool_ext[s, pl.ds(0, TILE), :] = jnp.zeros((TILE, POOL_CH), bf16)

    first = nrm.at[0, pl.ds(0, len(first_loads) * depth * LANES // width)]
    pltpu.make_async_copy(first, first, load_sem.at[0]).wait()
    k_all, v_all = kv_in[0], kv_in[1]
    first = jnp.concatenate([k_all[:, :HEAD_SIZE], v_all[:, :HEAD_SIZE]], axis=1)
    second = jnp.concatenate([k_all[:, HEAD_SIZE:], v_all[:, HEAD_SIZE:]], axis=1)
    held[me, 0] = jnp.where(y == 0, first, second)
    gain_load.wait()
    pl.semaphore_wait(barrier, 4 + has_up.astype(jnp.int32) + has_down.astype(jnp.int32))
    strip = 32

    def norm(i):
        tok_load(i).wait()
        for part in range(chunk // strip):
            at = pl.multiple_of(own_at(i) + part * strip, strip)
            v = tok[pl.ds(at, strip), :].astype(f32)
            scale = lax.rsqrt(jnp.mean(v * v, axis=-1, keepdims=True) + EPSILON)
            nrm[0, pl.ds(pl.multiple_of(c * half + at, strip), strip), :] = (v * scale * gain_v[...]).astype(bf16)
        if i == norm_order[0]:
            y_tok(0).start()
        tok_hop(i).start()

    def own_tokens():
        got_all(nrm.at[0, pl.ds(0, half)], tok_recv)
        for i in range(1, 4):
            y_tok(i).start()

    def y_service(i):
        y_tok(i).wait_recv()
        fwd(i).start()

    def project(s, r0, size, cols, shards, acc=None):
        for j in shards:
            w = held[j, cols[0]] if len(cols) == 1 else jnp.concatenate([held[j, b] for b in cols], axis=1)
            deep = slice(j * depth, (j + 1) * depth) if isinstance(j, int) else pl.ds(pl.multiple_of(j * depth, depth), depth)
            term = jnp.dot(nrm[s, r0 : r0 + size, deep], w, preferred_element_type=f32)
            acc = term if acc is None else acc + term
        return acc

    every = range(n)
    early, last = [me] + shard[:-1], shard[-1:]

    def halo_kv(s):
        return remote(
            kvb.at[s, pl.ds(rows, WINDOW)], kvb.at[s, pl.ds(0, WINDOW)], halo_send.at[s], halo_recv.at[s], {"sp": up}
        )

    def halo_pool(s):
        return remote(
            pool_ext.at[s, pl.ds(rows, TILE)],
            pool_ext.at[s, pl.ds(0, TILE)],
            halo_send.at[2 + s],
            halo_recv.at[2 + s],
            {"sp": up},
        )

    def send_halo(halo, s):
        @pl.when(has_up)
        def _():
            halo(s).start()

    def wait_halo(halo, s):
        @pl.when(has_down)
        def _():
            halo(s).wait_recv()

    def project_kv(s, r0, size):
        kvb[s, pl.ds(WINDOW + r0, size), :] = project(s, r0, size, [0], every).astype(bf16)

    def project_q(s, r0, size):
        qb[s, pl.ds(r0, size), :] = project(s, r0, size, [1, 2], every).astype(bf16)

    def begin_q(s, r0, size):
        acc_q[s, pl.ds(r0, size), :] = project(s, r0, size, [1, 2], early)

    def end_q(s, r0, size):
        qb[s, pl.ds(r0, size), :] = project(s, r0, size, [1, 2], last, acc_q[s, pl.ds(r0, size), :]).astype(bf16)

    def project_pool(s, r0, size):
        pool_ext[s, pl.ds(TILE + r0, size), :] = project(s, r0, size, [3, 4], every).astype(bf16)

    def begin_pool(s, r0, size):
        acc_p[s, pl.ds(r0, size), :] = project(s, r0, size, [3, 4], early)

    def end_pool(s, r0, size):
        done = project(s, r0, size, [3, 4], last, acc_p[s, pl.ds(r0, size), :])
        pool_ext[s, pl.ds(TILE + r0, size), :] = done.astype(bf16)

    def attend(s, b):
        base = b * WINDOW
        lane = lax.broadcasted_iota(jnp.int32, (WINDOW, LANES), 1)
        lgs = jnp.zeros((WINDOW, LANES), f32)
        i_pos = lax.broadcasted_iota(jnp.int32, (WINDOW, 2 * WINDOW), 0)
        k_pos = lax.broadcasted_iota(jnp.int32, (WINDOW, 2 * WINDOW), 1)
        allowed = (k_pos > i_pos) & (k_pos <= i_pos + WINDOW)
        if b == 0:
            allowed = allowed & (k_pos + (me * rows - WINDOW) >= 0)
        band = kvb[s, pl.ds(base, 2 * WINDOW), :]
        keys, vals = band[:, :HEAD_SIZE], band[:, HEAD_SIZE:]
        q = qb[s, pl.ds(base, WINDOW), :]
        q = jnp.concatenate([q[:, h * HEAD_SIZE : (h + 1) * HEAD_SIZE] for h in range(group)], axis=0)
        scores = lax.dot_general(q, keys, (((1,), (1,)), ((), ())), preferred_element_type=f32)
        probs = []
        for h in range(group):
            sink = sink_v[(2 * c + y) * group + h]
            sc = jnp.where(allowed, scores[h * WINDOW : (h + 1) * WINDOW] * HEAD_SIZE**-0.5, -jnp.inf)
            top = jnp.maximum(jnp.max(sc, axis=-1, keepdims=True), sink)
            w = jnp.exp(sc - top)
            total = jnp.sum(w, axis=-1, keepdims=True) + jnp.exp(sink - top)
            probs.append((w * (1.0 / total)).astype(bf16))
            lgs = jnp.where(lane == h, top + jnp.log(total), lgs)
        res = jnp.dot(jnp.concatenate(probs, axis=0), vals, preferred_element_type=f32)
        res = jnp.concatenate([res[h * WINDOW : (h + 1) * WINDOW] for h in range(group)], axis=1)
        mixed[s, pl.ds(base, WINDOW), pl.ds(0, q_cols)] = res.astype(bf16)
        logs[s, :, pl.ds(base, WINDOW)] = jnp.transpose(lgs)[: logs.shape[1]]

    def pool(s, part):
        base = part * half
        run = pool_ext[s, pl.ds(base, TILE + half), :].astype(f32)
        own = run[TILE:]
        trailing = jnp.zeros_like(run)
        span_here = jnp.int32(0)
        reach = 1
        for at, span in enumerate(POOL_SPANS):
            while reach < span:
                run = run + pltpu.roll(run, reach, 0)
                reach *= 2
            trailing = jnp.where(pool_index == at, run, trailing)
            span_here = jnp.where(pool_index == at, span, span_here)
        pos = me * rows + base + lax.broadcasted_iota(jnp.int32, (half, 1), 0)
        count = jnp.minimum(pos + 1, span_here).astype(f32)
        centred = (trailing[TILE:] / count - own).astype(bf16)
        product = jnp.dot(centred, mix_own[...], preferred_element_type=f32)
        mixed[s, pl.ds(base, half), pl.ds(q_cols, POOL_CH)] = (product * pgain_v[pool_index]).astype(bf16)

    def log_hop():
        return remote(logs.at[1], logs_got, log_send, log_recv, {"fs": across})

    order = [me] + shard
    wide = out_cols // 2

    def sum_n(part, i):
        u = i * 2 + part
        return remote(send_n.at[u], got_n.at[u], sumn_send, sumn_recv.at[u], {"tp": 1 - c})

    def sum_o(i):
        return remote(sent.at[i], got.at[i], sumo_send, sumo_recv.at[i], {"tp": 1 - c})

    def y_sum(part, i):
        return remote(
            y_part.at[i * 2 + part], y_got.at[i, c], yp_send, yp_recv.at[i], {"fs": across, "tp": part}
        )

    def out_far(part, i):
        u = i * 2 + part
        acc = jnp.dot(mixed[1, part * half : (part + 1) * half, :], wout[order[i]], preferred_element_type=f32)
        left, right = acc[:, :wide], acc[:, wide:]
        keep_n[u] = jnp.where(c == 0, left, right)
        send_n[u] = jnp.where(c == 0, right, left)
        sum_n(part, i).start()

    def pass_far(part, i):
        u = i * 2 + part
        sum_n(part, i).wait_recv()
        y_part[u] = (keep_n[u] + got_n[u]).astype(bf16)
        y_sum(part, i).start()

    def out_own(i):
        acc = jnp.dot(mixed[0], wout[order[i]], preferred_element_type=f32)
        low, high = acc[:half], acc[half:]
        mine[i] = jnp.where(c == 0, low, high)
        sent[i] = jnp.where(c == 0, high, low)
        sum_o(i).start()

    def finish(i):
        sum_o(i).wait_recv()
        got_all(y_got.at[i], yp_recv.at[i])
        there = jnp.concatenate([y_got[i, 0], y_got[i, 1]], axis=1).astype(f32)
        out_v[i] = (mine[i] + got[i] + there).astype(bf16)
        out_copy(i).start()

    def out_copy(i):
        cols = pl.ds(pl.multiple_of(order[i] * out_cols, out_cols), out_cols)
        return pltpu.make_async_copy(out_v.at[i], out.at[:, cols], out_sem.at[0])

    log_copy = pltpu.make_async_copy(log_v, log_out, out_sem.at[1])

    def send_log():
        log_hop().start()

    def write_log():
        log_hop().wait()
        own_logs, far_logs = logs[0, :group], logs_got[:group]
        log_v[...] = jnp.where(
            y == 0, jnp.concatenate([own_logs, far_logs], axis=0), jnp.concatenate([far_logs, own_logs], axis=0)
        )
        log_copy.start()

    def drain():
        for z in range(n):

            @pl.when(me == z)
            def _():
                if z < n - 1:
                    sent_all(bulk(n_pieces * (z + 1)), z_send.at[0])
                if z:
                    sent_all(bulk(n_pieces * (n - z)), z_send.at[1])

        sent_all(bulk(n_pieces * (n - 1)), x_send)
        for sem in (tok_send, ytok_send, fwd_send):
            sent_all(nrm.at[0, pl.ds(0, half)], sem)

        @pl.when(has_up)
        def _():
            for s in range(2):
                halo_kv(s).wait_send()
                halo_pool(s).wait_send()

    def ready(pieces, ks):
        got_all(bulk(len(pieces) * len(ks)), x_recv.at[x_group(pieces[0], ks[0])])

    def ready_out(k):
        got_all(bulk(OUT_CUTS), x_recv.at[x_group(n_in, k)])

    def arrived(i):
        fwd(i).wait_recv()

    def late_wait():
        for cp in late_loads:
            cp.wait()

    W = WINDOW
    send_end(1)
    send_inner(1)
    norm(2)
    norm(0)
    norm(1)
    norm(3)
    send_end(2)
    send_inner(2)
    send_inner(0)
    send_end(0)
    inner_slot(1, 0)
    inner_slot(1, 1)
    send_end(3)
    inner_slot(2, 0)
    send_end(4)
    end_slot(1, 0)
    inner_slot(2, 1)
    end_slot(2, 0)
    own_tokens()
    end_slot(0, 0)
    end_slot(1, 1)
    end_slot(2, 1)
    inner_slot(0, 1)
    end_slot(0, 1)
    inner_slot(0, 0)
    end_slot(1, 2)
    inner_slot(1, 2)
    y_service(0)
    late_wait()
    send_end(8)
    end_slot(2, 2)
    inner_slot(2, 2)
    inner_slot(0, 2)
    send_inner(4)
    send_inner(3)
    y_service(1)
    ready([1, 2], range(n - 2))
    begin_q(0, half, half)
    end_slot(0, 2)
    send_end(6)
    arrived(0)
    inner_slot(4, 0)
    inner_slot(4, 1)
    inner_slot(3, 1)
    inner_slot(3, 0)
    end_slot(4, 0)
    begin_q(0, 0, half)
    ready([1, 2], [n - 2])
    end_q(0, 0, half)
    end_slot(3, 0)
    inner_slot(4, 2)
    arrived(1)
    begin_q(1, W, 2 * W)
    ready([0], range(n - 1))
    project_kv(0, 0, half)
    end_q(0, half, half)
    end_slot(4, 1)
    send_end(5)
    inner_slot(3, 2)
    send_inner(5)
    project_kv(0, half, half)
    attend(0, 2)
    y_service(2)
    end_slot(3, 1)
    send_inner(6)
    send_end(7)
    send_inner(8)
    attend(0, 1)
    project_kv(1, W, 2 * W)
    end_slot(4, 2)
    attend(0, 3)
    arrived(2)
    project_kv(1, 3 * W, W)
    send_halo(halo_kv, 1)
    send_inner(7)
    inner_slot(5, 1)
    inner_slot(5, 0)
    end_slot(3, 2)
    end_q(1, W, 2 * W)
    attend(1, 2)
    ready([3, 4], range(n - 2))
    begin_pool(0, half, half)
    end_slot(5, 0)
    y_service(3)
    begin_q(1, 3 * W, W)
    end_q(1, 3 * W, W)
    attend(1, 3)
    end_slot(6, 0)
    begin_pool(1, half - TILE, half + TILE)
    ready([3, 4], [n - 2])
    end_pool(1, half - TILE, half + TILE)
    send_halo(halo_pool, 1)
    inner_slot(6, 0)
    pool(1, 1)
    out_far(1, 0)
    end_pool(0, half, half)
    send_halo(halo_pool, 0)
    inner_slot(7, 0)
    send_halo(halo_kv, 0)
    inner_slot(8, 0)
    inner_slot(6, 1)
    end_slot(8, 0)
    inner_slot(7, 1)
    inner_slot(8, 1)
    arrived(3)
    project_kv(1, 0, W)
    attend(1, 1)
    wait_halo(halo_kv, 1)
    project_q(1, 0, W)
    attend(1, 0)
    send_log()
    pass_far(1, 0)
    inner_slot(5, 2)
    end_slot(7, 0)
    project_pool(1, 0, half - TILE)
    wait_halo(halo_pool, 1)
    pool(1, 0)
    out_far(0, 0)
    end_slot(5, 1)
    begin_pool(0, 0, half)
    end_pool(0, 0, half)
    pool(0, 1)
    wait_halo(halo_pool, 0)
    pool(0, 0)
    inner_slot(7, 2)
    end_slot(6, 1)
    inner_slot(6, 2)
    ready_out(0)
    out_far(0, 1)
    inner_slot(8, 2)
    end_slot(7, 1)
    pass_far(0, 0)
    out_far(1, 1)
    wait_halo(halo_kv, 0)
    attend(0, 0)
    out_own(0)
    end_slot(8, 1)
    out_own(1)
    pass_far(0, 1)
    pass_far(1, 1)
    end_slot(5, 2)
    end_slot(7, 2)
    finish(0)
    ready_out(1)
    out_far(1, 2)
    out_far(0, 2)
    end_slot(6, 2)
    out_own(2)
    end_slot(8, 2)
    drain()
    write_log()
    pass_far(1, 2)
    pass_far(0, 2)
    finish(1)
    ready_out(2)
    out_far(0, 3)
    out_far(1, 3)
    out_own(3)
    pass_far(0, 3)
    pass_far(1, 3)
    finish(2)
    finish(3)
    sent_all(send_n, sumn_send)
    sent_all(sent, sumo_send)
    sent_all(y_part, yp_send)
    pltpu.make_async_copy(out, out, out_sem.at[0]).wait()
    log_copy.wait()


def fused_local(
    n,
    tokens,
    norm_gain,
    query_weight,
    key_matrix,
    value_matrix,
    pool_in_weight,
    head_sink_logit,
    pool_mix,
    pool_gain,
    attn_out_weight,
    pool_out_weight,
):
    _, half, width = tokens.shape
    rows = 2 * half
    depth, q_all = query_weight.shape
    heads = q_all // HEAD_SIZE
    kv_cols = key_matrix.shape[1]
    q_cols = q_all // 2
    out_cols = attn_out_weight.shape[1]
    n_in = 1 + 2 * (q_cols // LANES)
    pieces = n_in + OUT_CUTS
    bf16, f32 = jnp.bfloat16, jnp.float32
    dma = pltpu.SemaphoreType.DMA
    hbm = pl.BlockSpec(memory_space=pl.ANY)
    mixed, logs = pl.pallas_call(
        functools.partial(layer_kernel, n),
        out_shape=(
            jax.ShapeDtypeStruct((half, width), bf16),
            jax.ShapeDtypeStruct((heads, rows), f32),
        ),
        in_specs=[hbm] * 11,
        out_specs=(hbm, hbm),
        scratch_shapes=[
            pltpu.VMEM((n, n_in, depth, LANES), bf16),
            pltpu.VMEM((n, depth, out_cols), bf16),
            pltpu.VMEM((2, depth, kv_cols), bf16),
            pltpu.VMEM((half, width), bf16),
            pltpu.VMEM((1, width), f32),
            pltpu.VMEM((2 * 2, 1, POOL_CH), f32),
            pltpu.SMEM(head_sink_logit.shape, f32),
            pltpu.VMEM((n, half, out_cols), bf16),
            pltpu.VMEM((heads, rows), f32),
            pltpu.VMEM((2, rows, q_cols), f32),
            pltpu.VMEM((2, rows, POOL_CH), f32),
            pltpu.VMEM((2, rows, width), bf16),
            pltpu.VMEM((2, rows, q_cols), bf16),
            pltpu.VMEM((2, WINDOW + rows, kv_cols), bf16),
            pltpu.VMEM((2, TILE + rows, POOL_CH), bf16),
            pltpu.VMEM((2, rows, q_cols + POOL_CH), bf16),
            pltpu.VMEM((POOL_CH, POOL_CH), bf16),
            pltpu.VMEM((2, heads, rows), f32),
            pltpu.VMEM((heads, rows), f32),
            pltpu.VMEM((2 * n, half, out_cols // 2), f32),
            pltpu.VMEM((2 * n, half, out_cols // 2), f32),
            pltpu.VMEM((2 * n, half, out_cols // 2), f32),
            pltpu.VMEM((2 * n, half, out_cols // 2), bf16),
            pltpu.VMEM((n, 2, half, out_cols // 2), bf16),
            pltpu.VMEM((n, half, out_cols), f32),
            pltpu.VMEM((n, half, out_cols), f32),
            pltpu.VMEM((n, half, out_cols), f32),
            dma((2,)),
            dma,
            dma((pieces, n - 1)),
            dma((5 + n - 1,)),
            dma((7,)),
            dma((4,)),
            dma,
            dma,
            dma,
            dma((4,)),
            dma,
            dma((4,)),
            dma((4,)),
            dma((4,)),
            dma,
            dma((2 * n,)),
            dma,
            dma((n,)),
            dma,
            dma((n,)),
            dma,
            dma,
            dma((2,)),
        ],
        compiler_params=pltpu.CompilerParams(
            collective_id=0, has_side_effects=True, vmem_limit_bytes=60 * 1024 * 1024
        ),
    )(
        head_sink_logit,
        tokens[0],
        norm_gain.reshape(1, width),
        query_weight,
        key_matrix,
        value_matrix,
        pool_in_weight,
        pool_mix,
        pool_gain.reshape(-1, 1, POOL_CH),
        attn_out_weight,
        pool_out_weight,
    )
    return mixed[None], logs[None]


def fits(mesh, tokens, query_weight, key_matrix, pool_in_weight, attn_out_weight):
    n, f, c = mesh.shape["sp"], mesh.shape["fs"], mesh.shape["tp"]
    depth = query_weight.shape[0] // n
    rows = tokens.shape[1] // n
    q_cols, kv_cols, pool_cols = (w.shape[1] // c for w in (query_weight, key_matrix, pool_in_weight))
    return (
        n == 4
        and f == 4
        and c == 2
        and tokens.shape[0] == f
        and rows == 4 * WINDOW
        and kv_cols == LANES == 2 * HEAD_SIZE
        and q_cols == 4 * LANES
        and pool_cols == 2 * POOL_CH == q_cols
        and attn_out_weight.shape[1] == n * 4 * LANES
        and attn_out_weight.shape[0] // c == depth == q_cols
    )


def solution(mesh):
    in_specs = (
        P("fs", ("sp", "tp"), None),
        P(),
        P("sp", "tp"),
        P("sp", "tp"),
        P("sp", "tp"),
        P("sp", "tp"),
        P(),
        P(),
        P(),
        P("tp", "sp"),
        P("tp", "sp"),
    )
    out_specs = (P("fs", ("sp", "tp"), None), P("fs", "tp", "sp"))

    def step(*args):
        fused = fits(mesh, args[0], args[2], args[3], args[5], args[9])
        body = functools.partial(fused_local, mesh.shape["sp"]) if fused else local
        mapped = jax.shard_map(body, mesh=mesh, in_specs=in_specs, out_specs=out_specs, check_vma=False)
        return mapped(*args)

    return step
```

```python
import functools

import jax
import jax.numpy as jnp
from jax import lax
from jax.experimental import pallas as pl
from jax.experimental.pallas import tpu as pltpu
from jax.sharding import PartitionSpec as P

HEAD_SIZE = 64
WINDOW = 128
POOL_CH = 256


EPSILON = 1e-06
POOL_SPANS = (2, 4, 8, 16)


def passed_along(shard, axis, by):
    size = lax.axis_size(axis)
    pairs = [(i, i + by) for i in range(size) if 0 <= i + by < size]
    return lax.ppermute(shard, axis, pairs)


def windowed_attend(
    query_rows, key_rows, value_rows, key_tail, value_tail, sinks, kv_heads, group, first_pos
):
    rows = query_rows.shape[0]
    blocks = rows // WINDOW
    width = key_rows.shape[1]
    ext_keys = jnp.concatenate([key_tail, key_rows], 0)
    ext_values = jnp.concatenate([value_tail, value_rows], 0)

    def banded(table):
        return jnp.concatenate(
            [
                table[:rows].reshape(blocks, WINDOW, width),
                table[WINDOW:].reshape(blocks, WINDOW, width),
            ],
            axis=1,
        )

    band_keys = banded(ext_keys).reshape(blocks, 2 * WINDOW, kv_heads, HEAD_SIZE)
    band_values = banded(ext_values).reshape(blocks, 2 * WINDOW, kv_heads, HEAD_SIZE)
    query_blocks = query_rows.reshape(blocks, WINDOW, kv_heads, group, HEAD_SIZE)
    scores = jnp.einsum(
        "bqkgd,bskd->bkgqs", query_blocks, band_keys, preferred_element_type=jnp.float32
    ) * HEAD_SIZE ** (-0.5)
    query_pos = first_pos + jnp.arange(rows).reshape(blocks, WINDOW, 1)
    key_pos = (
        first_pos
        - WINDOW
        + jnp.arange(blocks).reshape(blocks, 1, 1) * WINDOW
        + jnp.arange(2 * WINDOW).reshape(1, 1, 2 * WINDOW)
    )
    offset = query_pos - key_pos
    allowed = (offset >= 0) & (offset < WINDOW) & (key_pos >= 0)
    scores = jnp.where(allowed[:, None, None], scores, -jnp.inf)
    sink_grid = sinks.reshape(1, kv_heads, group, 1, 1)
    top = jnp.maximum(jnp.max(scores, axis=-1, keepdims=True), sink_grid)
    weights = jnp.exp(scores - top)
    total = jnp.sum(weights, axis=-1, keepdims=True) + jnp.exp(sink_grid - top)
    probs = (weights / total).astype(jnp.bfloat16)
    mixed = jnp.einsum(
        "bkgqs,bskd->bqkgd", probs, band_values, preferred_element_type=jnp.float32
    ).astype(jnp.bfloat16)
    row_log_weight_sum = (top + jnp.log(total))[..., 0]
    return (
        mixed.reshape(rows, kv_heads * group * HEAD_SIZE),
        row_log_weight_sum.transpose(1, 2, 0, 3).reshape(kv_heads * group, rows),
    )


def pool_branch(pool_rows, pool_tail, mixing, scales, group_start, first_pos):
    rows = pool_rows.shape[0]
    columns = pool_rows.shape[1]
    pool_reach = max(POOL_SPANS)
    extended = jnp.concatenate([pool_tail, pool_rows], 0).astype(jnp.float32)
    group_index = group_start + jnp.arange(columns) // POOL_CH
    span_table = jnp.array(POOL_SPANS, jnp.int32)
    matches = group_index[:, None] == jnp.arange(len(POOL_SPANS))[None, :]
    span_of_col = jnp.sum(jnp.where(matches, span_table[None, :], 0), axis=1)
    trailing = jnp.zeros((rows, columns), jnp.float32)
    for lag in range(pool_reach):
        trailing = trailing + jnp.where(
            lag < span_of_col[None, :], extended[pool_reach - lag : pool_reach - lag + rows], 0.0
        )
    position = first_pos + jnp.arange(rows)
    count = jnp.minimum(position[:, None] + 1, span_of_col[None, :]).astype(jnp.float32)
    centred = (trailing / count - extended[pool_reach:]).astype(jnp.bfloat16)
    grouped = centred.reshape(rows, columns // POOL_CH, POOL_CH)
    product = jnp.einsum(
        "rgc,gcd->rgd", grouped, mixing, preferred_element_type=jnp.float32
    ).reshape(rows, columns)
    return (product * scales).astype(jnp.bfloat16)


def local(
    tokens,
    norm_gain,
    query_weight,
    key_matrix,
    value_matrix,
    pool_in_weight,
    head_sink_logit,
    pool_mix,
    pool_gain,
    attn_out_weight,
    pool_out_weight,
):
    tp_index = lax.axis_index("tp")
    sp_index = lax.axis_index("sp")
    q_cols = query_weight.shape[1]
    kv_cols = key_matrix.shape[1]
    pool_cols = pool_in_weight.shape[1]
    q_heads = q_cols // HEAD_SIZE
    kv_heads = kv_cols // HEAD_SIZE
    groups_dev = pool_cols // POOL_CH
    full_query, full_key, full_value, full_pool = (
        lax.all_gather(query_weight, "sp", axis=0, tiled=True),
        lax.all_gather(key_matrix, "sp", axis=0, tiled=True),
        lax.all_gather(value_matrix, "sp", axis=0, tiled=True),
        lax.all_gather(pool_in_weight, "sp", axis=0, tiled=True),
    )
    values_f = lax.all_gather(tokens[0], "tp", axis=0, tiled=True).astype(jnp.float32)
    scale = lax.rsqrt(jnp.mean(values_f * values_f, axis=-1, keepdims=True) + EPSILON)
    normed = (values_f * scale * norm_gain).astype(jnp.bfloat16)
    outputs = [
        jnp.dot(normed, weight, preferred_element_type=jnp.float32).astype(jnp.bfloat16)
        for weight in (full_query, full_key, full_value, full_pool)
    ]
    projected = jnp.concatenate(outputs, axis=1)
    rows = projected.shape[0]
    first_pos = sp_index * rows
    query_rows = projected[:, :q_cols]
    key_rows = projected[:, q_cols : q_cols + kv_cols]
    value_rows = projected[:, q_cols + kv_cols : q_cols + 2 * kv_cols]
    pool_rows = projected[:, q_cols + 2 * kv_cols :]
    pool_reach = max(POOL_SPANS)
    sinks = lax.dynamic_slice_in_dim(head_sink_logit, tp_index * q_heads, q_heads, 0)
    mixing = lax.dynamic_slice_in_dim(pool_mix, tp_index * groups_dev, groups_dev, 0)
    scales = lax.dynamic_slice_in_dim(pool_gain, tp_index * pool_cols, pool_cols, 0)
    key_tail, value_tail, pool_tail = passed_along(
        (key_rows[rows - WINDOW :], value_rows[rows - WINDOW :], pool_rows[rows - pool_reach :]),
        "sp",
        1,
    )
    attn_part, log_part = windowed_attend(
        query_rows,
        key_rows,
        value_rows,
        key_tail,
        value_tail,
        sinks,
        kv_heads,
        q_heads // kv_heads,
        first_pos,
    )
    pool_part = pool_branch(pool_rows, pool_tail, mixing, scales, tp_index * groups_dev, first_pos)
    half_attn, half_pool = (
        lax.all_gather(attn_out_weight, "sp", axis=1, tiled=True),
        lax.all_gather(pool_out_weight, "sp", axis=1, tiled=True),
    )
    result = lax.psum_scatter(
        jnp.dot(attn_part, half_attn, preferred_element_type=jnp.float32)
        + jnp.dot(pool_part, half_pool, preferred_element_type=jnp.float32),
        "tp",
        scatter_dimension=0,
        tiled=True,
    ).astype(jnp.bfloat16)
    return (result[None], log_part[None])


LANES = 128
TILE = 16
OUT_CUTS = 4
MESH_ID = pl.DeviceIdType.MESH


def nearest(n, step, me):
    tables = [sorted((j for j in range(n) if j != z), key=lambda j: (abs(j - z), j)) for z in range(n)]
    shard = jnp.int32(tables[0][step])
    for z in range(1, n):
        shard = jnp.where(me == z, tables[z][step], shard)
    return shard


def layer_kernel(
    n,
    sinks,
    tokens,
    gain,
    wq,
    wk,
    wv,
    wp,
    mix,
    pool_gain,
    wao,
    wpo,
    out,
    log_out,
    held,
    wout,
    kv_in,
    tok,
    gain_v,
    pgain_v,
    sink_v,
    out_v,
    log_v,
    acc_q,
    acc_p,
    nrm,
    qb,
    kvb,
    pool_ext,
    mixed,
    mix_own,
    logs,
    logs_got,
    keep_n,
    send_n,
    got_n,
    y_part,
    y_got,
    keep_m,
    send_m,
    got_m,
    y_part_m,
    y_got_m,
    mine,
    sent,
    got,
    z_send,
    x_send,
    z_recv,
    x_recv,
    load_sem,
    tok_sem,
    tok_send,
    tok_recv,
    ytok_send,
    ytok_recv,
    fwd_send,
    fwd_recv,
    halo_send,
    halo_recv,
    sumn_send,
    sumn_recv,
    sumo_send,
    sumo_recv,
    yp_send,
    yp_recv,
    log_send,
    log_recv,
    out_sem,
):
    me = lax.axis_index("sp")
    f = lax.axis_index("fs")
    c = lax.axis_index("tp")
    f32, bf16 = jnp.float32, jnp.bfloat16
    half, width = tokens.shape
    rows = 2 * half
    depth = wq.shape[0]
    part_rows = depth // 2
    q_cols = wq.shape[1] // 2
    group = q_cols // HEAD_SIZE
    out_cols = wao.shape[1]
    n_in = held.shape[1] + 1
    n_pieces = n_in + OUT_CUTS
    n_units = n_pieces - 1
    chunk = half // 4
    blocks = rows // WINDOW
    y, x = f // 2, lax.rem(f, 2)
    beside = f + 1 - 2 * x
    across = lax.rem(f + 2, 4)
    up, down = me + 1, me - 1
    has_up, has_down = me < n - 1, me > 0
    inner = has_up & has_down

    def at_cols(ref, i):
        return ref.at[:, pl.ds(pl.multiple_of(y * q_cols + i * LANES, LANES), LANES)]

    y_rows = pl.ds(pl.multiple_of(y * part_rows, part_rows), part_rows)
    pool_index = 2 * c + y
    norm_order = (2, 0, 1, 3)

    def own_chunk(i, side):
        first = (3, 1, 2, 0) if side == 0 else (0, 2, 1, 3)
        return first[i] * chunk

    def own_at(i):
        return pl.multiple_of(jnp.where(c == 0, own_chunk(i, 0), own_chunk(i, 1)), chunk)

    def tok_load(i):
        at = pl.ds(own_at(i), chunk)
        return pltpu.make_async_copy(tokens.at[at], tok.at[at], tok_sem.at[i])

    first_loads = [
        pltpu.make_async_copy(wk, kv_in.at[0], load_sem.at[0]),
        pltpu.make_async_copy(wv, kv_in.at[1], load_sem.at[0]),
    ]
    for i in range(2):
        first_loads.append(pltpu.make_async_copy(at_cols(wq, i), held.at[me, 1 + i], load_sem.at[0]))
    for i in range(2):
        first_loads.append(pltpu.make_async_copy(at_cols(wp, i), held.at[me, 3 + i], load_sem.at[0]))
    out_loads = []
    for i in range(out_cols // LANES):
        for side, w in enumerate((wao, wpo)):
            to = wout.at[me, i, pl.ds(side * part_rows, part_rows)]
            out_loads.append(pltpu.make_async_copy(w.at[y_rows, pl.ds(i * LANES, LANES)], to, load_sem.at[1]))
    late_loads = [
        pltpu.make_async_copy(mix.at[pool_index], mix_own, load_sem.at[3]),
        pltpu.make_async_copy(pool_gain, pgain_v, load_sem.at[4]),
        pltpu.make_async_copy(sinks, sink_v, load_sem.at[5]),
    ]
    gain_load = pltpu.make_async_copy(gain, gain_v, load_sem.at[6])
    barrier = pltpu.get_barrier_semaphore()
    for peer in ({"tp": 1 - c}, {"fs": beside}, {"fs": across}, {"fs": across, "tp": 1 - c}):
        pl.semaphore_signal(barrier, inc=1, device_id=peer, device_id_type=MESH_ID)

    @pl.when(has_up)
    def _():
        pl.semaphore_signal(barrier, inc=1, device_id={"sp": up}, device_id_type=MESH_ID)

    @pl.when(has_down)
    def _():
        pl.semaphore_signal(barrier, inc=1, device_id={"sp": down}, device_id_type=MESH_ID)

    for cp in first_loads[:2]:
        cp.start()
    tok_load(norm_order[0]).start()
    gain_load.start()
    for cp in first_loads[2:]:
        cp.start()
    for i in norm_order[1:]:
        tok_load(i).start()
    for cp in out_loads + late_loads:
        cp.start()

    def remote(src, dst, send, recv, to):
        return pltpu.make_async_remote_copy(src, dst, send, recv, device_id=to, device_id_type=MESH_ID)

    def piece(s, j, part):
        if s < n_in - 2:
            return held.at[j, s, pl.ds(pl.multiple_of(part * part_rows, part_rows), part_rows)]
        if s < n_in:
            size = part_rows // 2
            return held.at[j, n_in - 2, pl.ds(pl.multiple_of(part * part_rows + (s - n_in + 2) * size, size), size)]
        block, side = divmod(s - n_in, 2)
        return wout.at[j, 2 * part + block, pl.ds(side * part_rows, part_rows)]

    def bulk(count):
        return nrm.at[0, pl.ds(0, count * part_rows * LANES // width)]

    def sent_all(ref, sem):
        pltpu.make_async_remote_copy(ref, ref, sem, sem, device_id={"tp": 1 - c}, device_id_type=MESH_ID).wait_send()

    def got_all(ref, sem):
        pltpu.make_async_remote_copy(ref, ref, sem, sem, device_id={"tp": 1 - c}, device_id_type=MESH_ID).wait_recv()

    def z_hop(s, j, way):
        block = piece(s, j, x)
        to = me if way is None else jnp.where(way == 0, up, down)
        slot = z_recv.at[s, lax.rem(j - to + n, n) - 1]
        return remote(block, block, z_send.at[0 if way is None else way], slot, {"sp": to})

    def x_group(s, k):
        if s >= n_in:
            return 5 + k
        return 0 if s == 0 else 1 + 2 * min((s - 1) // 2, 1) + k // (n - 2)

    def x_hop(s, k):
        block = piece(s, shard[k], x)
        return remote(block, block, x_send, x_recv.at[x_group(s, k)], {"fs": beside})

    def onward(j):
        return jnp.where(j < me, 0, 1), ((j < me) & has_up) | ((j > me) & has_down)

    def own_send(s):
        @pl.when(has_up)
        def _():
            z_hop(s, me, 0).start()

        @pl.when(has_down)
        def _():
            z_hop(s, me, 1).start()

    shard = [nearest(n, k, me) for k in range(n - 1)]
    def pass_on(s, k):
        j = shard[k]
        z_hop(s, j, None).wait_recv()
        way, more = onward(j)

        @pl.when(more)
        def _():
            z_hop(s, j, way).start()

        x_hop(s, k).start()

    def inner_slot(s, k):
        @pl.when(inner)
        def _():
            pass_on(s, k)

    def end_slot(s, k):
        @pl.when(jnp.logical_not(inner))
        def _():
            pass_on(s, k)

    def send_inner(s):
        @pl.when(inner)
        def _():
            own_send(s)

    def send_end(s):
        @pl.when(jnp.logical_not(inner))
        def _():
            own_send(s)

    def pick(a, b):
        return pl.ds(pl.multiple_of(jnp.where(c == 0, a, b), chunk), chunk)

    def tok_hop(i):
        block = nrm.at[0, pick(own_chunk(i, 0), half + own_chunk(i, 1))]
        return remote(block, block, tok_send, tok_recv, {"tp": 1 - c})

    low_order = (2, 4, 6, 0)
    high_order = (5, 3, 7, 1)

    def y_tok(i):
        where = pick(low_order[i] * chunk, high_order[i] * chunk)
        return remote(nrm.at[0, where], nrm.at[1, where], ytok_send, ytok_recv.at[i], {"fs": across})

    def fwd(i):
        block = nrm.at[1, pick(low_order[i] * chunk, high_order[i] * chunk)]
        return remote(block, block, fwd_send, fwd_recv.at[i], {"tp": 1 - c})

    @pl.when(me == 0)
    def _():
        for s in range(2):
            kvb[s, pl.ds(0, WINDOW), :] = jnp.zeros((WINDOW, kvb.shape[2]), bf16)
            pool_ext[s, pl.ds(0, TILE), :] = jnp.zeros((TILE, POOL_CH), bf16)

    first = nrm.at[0, pl.ds(0, len(first_loads) * depth * LANES // width)]
    pltpu.make_async_copy(first, first, load_sem.at[0]).wait()
    k_all, v_all = kv_in[0], kv_in[1]
    first = jnp.concatenate([k_all[:, :HEAD_SIZE], v_all[:, :HEAD_SIZE]], axis=1)
    second = jnp.concatenate([k_all[:, HEAD_SIZE:], v_all[:, HEAD_SIZE:]], axis=1)
    held[me, 0] = jnp.where(y == 0, first, second)
    gain_load.wait()
    pl.semaphore_wait(barrier, 4 + has_up.astype(jnp.int32) + has_down.astype(jnp.int32))
    strip = 32

    def norm(i):
        tok_load(i).wait()
        for part in range(chunk // strip):
            at = pl.multiple_of(own_at(i) + part * strip, strip)
            v = tok[pl.ds(at, strip), :].astype(f32)
            scale = lax.rsqrt(jnp.mean(v * v, axis=-1, keepdims=True) + EPSILON)
            nrm[0, pl.ds(pl.multiple_of(c * half + at, strip), strip), :] = (v * scale * gain_v[...]).astype(bf16)
        if i == norm_order[0]:
            y_tok(0).start()
        tok_hop(i).start()

    def own_tokens():
        got_all(nrm.at[0, pl.ds(0, half)], tok_recv)
        for i in range(1, 4):
            y_tok(i).start()

    def y_service(i):
        y_tok(i).wait_recv()
        fwd(i).start()

    def project(s, r0, size, cols, shards, acc=None):
        for j in shards:
            w = held[j, cols[0]] if len(cols) == 1 else jnp.concatenate([held[j, b] for b in cols], axis=1)
            deep = slice(j * depth, (j + 1) * depth) if isinstance(j, int) else pl.ds(pl.multiple_of(j * depth, depth), depth)
            term = jnp.dot(nrm[s, r0 : r0 + size, deep], w, preferred_element_type=f32)
            acc = term if acc is None else acc + term
        return acc

    every = range(n)
    early, last = [me] + shard[:-1], shard[-1:]

    def halo_kv(s):
        return remote(
            kvb.at[s, pl.ds(rows, WINDOW)], kvb.at[s, pl.ds(0, WINDOW)], halo_send.at[s], halo_recv.at[s], {"sp": up}
        )

    def halo_pool(s):
        return remote(
            pool_ext.at[s, pl.ds(rows, TILE)],
            pool_ext.at[s, pl.ds(0, TILE)],
            halo_send.at[2 + s],
            halo_recv.at[2 + s],
            {"sp": up},
        )

    def send_halo(halo, s):
        @pl.when(has_up)
        def _():
            halo(s).start()

    def wait_halo(halo, s):
        @pl.when(has_down)
        def _():
            halo(s).wait_recv()

    def project_kv(s, r0, size):
        kvb[s, pl.ds(WINDOW + r0, size), :] = project(s, r0, size, [0], every).astype(bf16)

    def project_q(s, r0, size):
        qb[s, pl.ds(r0, size), :] = project(s, r0, size, [1, 2], every).astype(bf16)

    def begin_q(s, r0, size):
        acc_q[s, pl.ds(r0, size), :] = project(s, r0, size, [1, 2], early)

    def end_q(s, r0, size):
        qb[s, pl.ds(r0, size), :] = project(s, r0, size, [1, 2], last, acc_q[s, pl.ds(r0, size), :]).astype(bf16)

    def project_pool(s, r0, size):
        pool_ext[s, pl.ds(TILE + r0, size), :] = project(s, r0, size, [3, 4], every).astype(bf16)

    def begin_pool(s, r0, size):
        acc_p[s, pl.ds(r0, size), :] = project(s, r0, size, [3, 4], early)

    def end_pool(s, r0, size):
        done = project(s, r0, size, [3, 4], last, acc_p[s, pl.ds(r0, size), :])
        pool_ext[s, pl.ds(TILE + r0, size), :] = done.astype(bf16)

    def attend(s, b):
        base = b * WINDOW
        lane = lax.broadcasted_iota(jnp.int32, (WINDOW, LANES), 1)
        lgs = jnp.zeros((WINDOW, LANES), f32)
        i_pos = lax.broadcasted_iota(jnp.int32, (WINDOW, 2 * WINDOW), 0)
        k_pos = lax.broadcasted_iota(jnp.int32, (WINDOW, 2 * WINDOW), 1)
        allowed = (k_pos > i_pos) & (k_pos <= i_pos + WINDOW)
        if b == 0:
            allowed = allowed & (k_pos + (me * rows - WINDOW) >= 0)
        band = kvb[s, pl.ds(base, 2 * WINDOW), :]
        keys, vals = band[:, :HEAD_SIZE], band[:, HEAD_SIZE:]
        q = qb[s, pl.ds(base, WINDOW), :]
        q = jnp.concatenate([q[:, h * HEAD_SIZE : (h + 1) * HEAD_SIZE] for h in range(group)], axis=0)
        scores = lax.dot_general(q, keys, (((1,), (1,)), ((), ())), preferred_element_type=f32)
        probs = []
        for h in range(group):
            sink = sink_v[(2 * c + y) * group + h]
            sc = jnp.where(allowed, scores[h * WINDOW : (h + 1) * WINDOW] * HEAD_SIZE**-0.5, -jnp.inf)
            top = jnp.maximum(jnp.max(sc, axis=-1, keepdims=True), sink)
            w = jnp.exp(sc - top)
            total = jnp.sum(w, axis=-1, keepdims=True) + jnp.exp(sink - top)
            probs.append((w * (1.0 / total)).astype(bf16))
            lgs = jnp.where(lane == h, top + jnp.log(total), lgs)
        res = jnp.dot(jnp.concatenate(probs, axis=0), vals, preferred_element_type=f32)
        res = jnp.concatenate([res[h * WINDOW : (h + 1) * WINDOW] for h in range(group)], axis=1)
        mixed[s, pl.ds(base, WINDOW), pl.ds(0, q_cols)] = res.astype(bf16)
        logs[s, :, pl.ds(base, WINDOW)] = jnp.transpose(lgs)[: logs.shape[1]]

    def pool(s, part):
        base = part * half
        run = pool_ext[s, pl.ds(base, TILE + half), :].astype(f32)
        own = run[TILE:]
        trailing = jnp.zeros_like(run)
        span_here = jnp.int32(0)
        reach = 1
        for at, span in enumerate(POOL_SPANS):
            while reach < span:
                run = run + pltpu.roll(run, reach, 0)
                reach *= 2
            trailing = jnp.where(pool_index == at, run, trailing)
            span_here = jnp.where(pool_index == at, span, span_here)
        pos = me * rows + base + lax.broadcasted_iota(jnp.int32, (half, 1), 0)
        count = jnp.minimum(pos + 1, span_here).astype(f32)
        centred = (trailing[TILE:] / count - own).astype(bf16)
        product = jnp.dot(centred, mix_own[...], preferred_element_type=f32)
        mixed[s, pl.ds(base, half), pl.ds(q_cols, POOL_CH)] = (product * pgain_v[pool_index]).astype(bf16)

    def log_hop():
        return remote(logs.at[1], logs_got, log_send, log_recv, {"fs": across})

    order = [me] + shard

    def unit(part, i, g):
        return part if i == 0 else 4 * (i - 1) + 2 * g + part

    def sum_n(part, i, g):
        u = unit(part, i, g)
        a, b = (send_n, got_n) if i == 0 else (send_m, got_m)
        return remote(a.at[u], b.at[u], sumn_send.at[min(i, 1)], sumn_recv.at[u + 2 * min(i, 1)], {"tp": 1 - c})

    def all_cols(j):
        return jnp.concatenate([wout[j, i] for i in range(out_cols // LANES)], axis=1)

    def sum_o(i):
        return remote(sent.at[i], got.at[i], sumo_send, sumo_recv.at[i], {"tp": 1 - c})

    def y_sum(part, i, g):
        u = unit(part, i, g)
        src, dst = (y_part.at[u], y_got.at[c]) if i == 0 else (y_part_m.at[u], y_got_m.at[i - 1, g, c])
        return remote(src, dst, yp_send.at[min(i, 1)], yp_recv.at[i], {"fs": across, "tp": part})

    def out_far(part, i, g):
        u = unit(part, i, g)
        j = order[i]
        keep, send = (keep_n, send_n) if i == 0 else (keep_m, send_m)
        if i == 0:
            w = all_cols(j)
        else:
            first = 2 * (x if g == 0 else 1 - x)
            w = jnp.concatenate([wout[j, first], wout[j, first + 1]], axis=1)
        acc = jnp.dot(mixed[1, part * half : (part + 1) * half, :], w, preferred_element_type=f32)
        across_cols = acc.shape[1] // 2
        left, right = acc[:, :across_cols], acc[:, across_cols:]
        keep[u] = jnp.where(c == 0, left, right)
        send[u] = jnp.where(c == 0, right, left).astype(bf16)
        sum_n(part, i, g).start()

    def pass_far(part, i, g):
        u = unit(part, i, g)
        keep, there, to = (keep_n, got_n, y_part) if i == 0 else (keep_m, got_m, y_part_m)
        sum_n(part, i, g).wait_recv()
        to[u] = (keep[u] + there[u].astype(f32)).astype(bf16)
        y_sum(part, i, g).start()

    def out_own(i):
        acc = jnp.dot(mixed[0], all_cols(order[i]), preferred_element_type=f32)
        low, high = acc[:half], acc[half:]
        mine[i] = jnp.where(c == 0, low, high)
        sent[i] = jnp.where(c == 0, high, low)
        sum_o(i).start()

    def finish(i):
        sum_o(i).wait_recv()
        if i == 0:
            got_all(y_got, yp_recv.at[i])
            there = jnp.concatenate([y_got[0], y_got[1]], axis=1).astype(f32)
        else:
            got_all(y_got_m.at[i - 1], yp_recv.at[i])
            near = [y_got_m[i - 1, 0, 0], y_got_m[i - 1, 0, 1]]
            other = [y_got_m[i - 1, 1, 0], y_got_m[i - 1, 1, 1]]
            there = jnp.where(
                x == 0, jnp.concatenate(near + other, axis=1), jnp.concatenate(other + near, axis=1)
            ).astype(f32)
        out_v[i] = (mine[i] + got[i] + there).astype(bf16)
        out_copy(i).start()

    def out_copy(i):
        cols = pl.ds(pl.multiple_of(order[i] * out_cols, out_cols), out_cols)
        return pltpu.make_async_copy(out_v.at[i], out.at[:, cols], out_sem.at[0])

    log_copy = pltpu.make_async_copy(log_v, log_out, out_sem.at[1])

    def send_log():
        log_hop().start()

    def write_log():
        log_hop().wait()
        own_logs, far_logs = logs[0, :group], logs_got[:group]
        log_v[...] = jnp.where(
            y == 0, jnp.concatenate([own_logs, far_logs], axis=0), jnp.concatenate([far_logs, own_logs], axis=0)
        )
        log_copy.start()

    def drain():
        for z in range(n):

            @pl.when(me == z)
            def _():
                if z < n - 1:
                    sent_all(bulk(n_units * (z + 1)), z_send.at[0])
                if z:
                    sent_all(bulk(n_units * (n - z)), z_send.at[1])

        sent_all(bulk(n_units * (n - 1)), x_send)
        for sem in (tok_send, ytok_send, fwd_send):
            sent_all(nrm.at[0, pl.ds(0, half)], sem)

        @pl.when(has_up)
        def _():
            for s in range(2):
                halo_kv(s).wait_send()
                halo_pool(s).wait_send()

    def ready(pieces, ks):
        got_all(bulk(len(pieces) * len(ks)), x_recv.at[x_group(pieces[0], ks[0])])

    def ready_out(k):
        got_all(bulk(OUT_CUTS), x_recv.at[x_group(n_in, k)])

    def arrived(i):
        fwd(i).wait_recv()

    def late_wait():
        pltpu.make_async_copy(wout.at[me], wout.at[me], load_sem.at[1]).wait()
        for cp in late_loads:
            cp.wait()

    W = WINDOW
    send_end(1)
    send_inner(1)
    send_inner(0)
    send_inner(4)
    send_end(0)
    norm(2)
    norm(0)
    norm(1)
    norm(3)
    send_end(5)
    send_inner(2)
    inner_slot(1, 1)
    send_end(4)
    inner_slot(1, 0)
    late_wait()
    send_end(8)
    inner_slot(0, 0)
    send_end(2)
    end_slot(1, 0)
    inner_slot(0, 1)
    send_inner(3)
    own_tokens()
    send_inner(5)
    end_slot(0, 0)
    send_end(3)
    inner_slot(1, 2)
    inner_slot(0, 2)
    end_slot(4, 0)
    end_slot(2, 0)
    end_slot(1, 1)
    end_slot(0, 1)
    end_slot(3, 0)
    inner_slot(2, 0)
    inner_slot(2, 1)
    inner_slot(4, 1)
    end_slot(5, 0)
    inner_slot(4, 0)
    send_end(7)
    inner_slot(2, 2)
    end_slot(1, 2)
    end_slot(0, 2)
    end_slot(2, 1)
    inner_slot(5, 0)
    inner_slot(3, 0)
    inner_slot(5, 1)
    y_service(1)
    inner_slot(3, 1)
    send_end(9)
    end_slot(4, 1)
    y_service(0)
    send_end(6)
    inner_slot(4, 2)
    inner_slot(5, 2)
    end_slot(2, 2)
    ready([0], range(n - 1))
    project_kv(0, 0, half)
    end_slot(5, 1)
    arrived(1)
    arrived(0)
    project_kv(1, W, 2 * W)
    inner_slot(3, 2)
    send_inner(7)
    end_slot(3, 1)
    send_inner(8)
    ready([1, 2], range(n - 2))
    begin_q(0, half, half)
    y_service(2)
    begin_q(0, 0, half)
    end_slot(4, 2)
    send_inner(6)
    begin_q(1, W, 2 * W)
    project_kv(0, half, half)
    end_slot(5, 2)
    ready([1, 2], [n - 2])
    end_q(0, half, half)
    attend(0, 3)
    end_slot(3, 2)
    attend(0, 2)
    send_inner(9)
    inner_slot(7, 1)
    arrived(2)
    project_kv(1, 3 * W, W)
    send_halo(halo_kv, 1)
    inner_slot(7, 0)
    end_q(1, W, 2 * W)
    attend(1, 2)
    end_slot(7, 0)
    inner_slot(8, 1)
    y_service(3)
    begin_q(1, 3 * W, W)
    end_q(1, 3 * W, W)
    attend(1, 3)
    ready([3, 4], range(n - 2))
    begin_pool(1, half - TILE, half + TILE)
    ready([3, 4], [n - 2])
    end_pool(1, half - TILE, half + TILE)
    pool(1, 1)
    out_far(1, 0, 0)
    send_halo(halo_pool, 1)
    inner_slot(6, 0)
    end_slot(6, 0)
    end_q(0, 0, half)
    arrived(3)
    project_q(1, 0, W)
    inner_slot(8, 0)
    end_slot(8, 0)
    inner_slot(9, 0)
    end_slot(9, 0)
    out_far(1, 1, 0)
    inner_slot(6, 1)
    project_kv(1, 0, W)
    attend(1, 1)
    pass_far(1, 0, 0)
    wait_halo(halo_kv, 1)
    attend(1, 0)
    send_log()
    pass_far(1, 1, 0)
    send_halo(halo_kv, 0)
    inner_slot(9, 1)
    end_slot(7, 1)
    project_pool(1, 0, half - TILE)
    wait_halo(halo_pool, 1)
    pool(1, 0)
    out_far(0, 0, 0)
    begin_pool(0, half, half)
    end_pool(0, half, half)
    send_halo(halo_pool, 0)
    end_slot(6, 1)
    out_far(0, 1, 0)
    inner_slot(7, 2)
    inner_slot(6, 2)
    begin_pool(0, 0, half)
    end_pool(0, 0, half)
    pool(0, 1)
    end_slot(8, 1)
    inner_slot(8, 2)
    pass_far(0, 0, 0)
    attend(0, 1)
    pass_far(0, 1, 0)
    inner_slot(9, 2)
    end_slot(9, 1)
    out_far(1, 2, 0)
    ready_out(0)
    out_far(1, 1, 1)
    out_far(0, 1, 1)
    out_far(0, 2, 0)
    wait_halo(halo_pool, 0)
    pool(0, 0)
    wait_halo(halo_kv, 0)
    attend(0, 0)
    out_own(0)
    pass_far(1, 1, 1)
    end_slot(7, 2)
    write_log()
    pass_far(0, 1, 1)
    pass_far(1, 2, 0)
    pass_far(0, 2, 0)
    out_own(1)
    end_slot(6, 2)
    end_slot(8, 2)
    ready_out(1)
    out_far(0, 2, 1)
    out_far(1, 2, 1)
    finish(0)
    end_slot(9, 2)
    out_far(0, 3, 0)
    out_far(1, 3, 0)
    out_own(2)
    pass_far(0, 2, 1)
    pass_far(1, 2, 1)
    pass_far(0, 3, 0)
    pass_far(1, 3, 0)
    finish(1)
    ready_out(2)
    out_far(1, 3, 1)
    out_far(0, 3, 1)
    out_own(3)
    pass_far(1, 3, 1)
    pass_far(0, 3, 1)
    drain()
    finish(2)
    finish(3)
    sent_all(send_n, sumn_send.at[0])
    sent_all(send_m, sumn_send.at[1])
    sent_all(sent, sumo_send)
    sent_all(y_part, yp_send.at[0])
    sent_all(y_part_m, yp_send.at[1])
    pltpu.make_async_copy(out, out, out_sem.at[0]).wait()
    log_copy.wait()


def fused_local(
    n,
    tokens,
    norm_gain,
    query_weight,
    key_matrix,
    value_matrix,
    pool_in_weight,
    head_sink_logit,
    pool_mix,
    pool_gain,
    attn_out_weight,
    pool_out_weight,
):
    _, half, width = tokens.shape
    rows = 2 * half
    depth, q_all = query_weight.shape
    heads = q_all // HEAD_SIZE
    kv_cols = key_matrix.shape[1]
    q_cols = q_all // 2
    out_cols = attn_out_weight.shape[1]
    n_in = 1 + 2 * (q_cols // LANES)
    pieces = n_in + 1 + OUT_CUTS
    bf16, f32 = jnp.bfloat16, jnp.float32
    dma = pltpu.SemaphoreType.DMA
    hbm = pl.BlockSpec(memory_space=pl.ANY)
    mixed, logs = pl.pallas_call(
        functools.partial(layer_kernel, n),
        out_shape=(
            jax.ShapeDtypeStruct((half, width), bf16),
            jax.ShapeDtypeStruct((heads, rows), f32),
        ),
        in_specs=[hbm] * 11,
        out_specs=(hbm, hbm),
        scratch_shapes=[
            pltpu.VMEM((n, n_in, depth, LANES), bf16),
            pltpu.VMEM((n, out_cols // LANES, depth, LANES), bf16),
            pltpu.VMEM((2, depth, kv_cols), bf16),
            pltpu.VMEM((half, width), bf16),
            pltpu.VMEM((1, width), f32),
            pltpu.VMEM((2 * 2, 1, POOL_CH), f32),
            pltpu.SMEM(head_sink_logit.shape, f32),
            pltpu.VMEM((n, half, out_cols), bf16),
            pltpu.VMEM((heads, rows), f32),
            pltpu.VMEM((2, rows, q_cols), f32),
            pltpu.VMEM((2, rows, POOL_CH), f32),
            pltpu.VMEM((2, rows, width), bf16),
            pltpu.VMEM((2, rows, q_cols), bf16),
            pltpu.VMEM((2, WINDOW + rows, kv_cols), bf16),
            pltpu.VMEM((2, TILE + rows, POOL_CH), bf16),
            pltpu.VMEM((2, rows, q_cols + POOL_CH), bf16),
            pltpu.VMEM((POOL_CH, POOL_CH), bf16),
            pltpu.VMEM((2, heads, rows), f32),
            pltpu.VMEM((heads, rows), f32),
            pltpu.VMEM((2, half, out_cols // 2), f32),
            pltpu.VMEM((2, half, out_cols // 2), bf16),
            pltpu.VMEM((2, half, out_cols // 2), bf16),
            pltpu.VMEM((2, half, out_cols // 2), bf16),
            pltpu.VMEM((2, half, out_cols // 2), bf16),
            pltpu.VMEM((4 * (n - 1), half, out_cols // 4), f32),
            pltpu.VMEM((4 * (n - 1), half, out_cols // 4), bf16),
            pltpu.VMEM((4 * (n - 1), half, out_cols // 4), bf16),
            pltpu.VMEM((4 * (n - 1), half, out_cols // 4), bf16),
            pltpu.VMEM((n - 1, 2, 2, half, out_cols // 4), bf16),
            pltpu.VMEM((n, half, out_cols), f32),
            pltpu.VMEM((n, half, out_cols), f32),
            pltpu.VMEM((n, half, out_cols), f32),
            dma((2,)),
            dma,
            dma((pieces, n - 1)),
            dma((5 + n - 1,)),
            dma((7,)),
            dma((4,)),
            dma,
            dma,
            dma,
            dma((4,)),
            dma,
            dma((4,)),
            dma((4,)),
            dma((4,)),
            dma((2,)),
            dma((2 + 4 * (n - 1),)),
            dma,
            dma((n,)),
            dma((2,)),
            dma((n,)),
            dma,
            dma,
            dma((2,)),
        ],
        compiler_params=pltpu.CompilerParams(
            collective_id=0, has_side_effects=True, vmem_limit_bytes=60 * 1024 * 1024
        ),
    )(
        head_sink_logit,
        tokens[0],
        norm_gain.reshape(1, width),
        query_weight,
        key_matrix,
        value_matrix,
        pool_in_weight,
        pool_mix,
        pool_gain.reshape(-1, 1, POOL_CH),
        attn_out_weight,
        pool_out_weight,
    )
    return mixed[None], logs[None]


def fits(mesh, tokens, query_weight, key_matrix, pool_in_weight, attn_out_weight):
    n, f, c = mesh.shape["sp"], mesh.shape["fs"], mesh.shape["tp"]
    depth = query_weight.shape[0] // n
    rows = tokens.shape[1] // n
    q_cols, kv_cols, pool_cols = (w.shape[1] // c for w in (query_weight, key_matrix, pool_in_weight))
    return (
        n == 4
        and f == 4
        and c == 2
        and tokens.shape[0] == f
        and rows == 4 * WINDOW
        and kv_cols == LANES == 2 * HEAD_SIZE
        and q_cols == 4 * LANES
        and pool_cols == 2 * POOL_CH == q_cols
        and attn_out_weight.shape[1] == n * 4 * LANES
        and attn_out_weight.shape[0] // c == depth == q_cols
    )


def solution(mesh):
    in_specs = (
        P("fs", ("sp", "tp"), None),
        P(),
        P("sp", "tp"),
        P("sp", "tp"),
        P("sp", "tp"),
        P("sp", "tp"),
        P(),
        P(),
        P(),
        P("tp", "sp"),
        P("tp", "sp"),
    )
    out_specs = (P("fs", ("sp", "tp"), None), P("fs", "tp", "sp"))

    def step(*args):
        fused = fits(mesh, args[0], args[2], args[3], args[5], args[9])
        body = functools.partial(fused_local, mesh.shape["sp"]) if fused else local
        mapped = jax.shard_map(body, mesh=mesh, in_specs=in_specs, out_specs=out_specs, check_vma=False)
        return mapped(*args)

    return step
```

```python
import functools

import jax
import jax.numpy as jnp
from jax import lax
from jax.experimental import pallas as pl
from jax.experimental.pallas import tpu as pltpu
from jax.sharding import PartitionSpec as P

HEAD_SIZE = 64
WINDOW = 128
POOL_CH = 256


EPSILON = 1e-06
POOL_SPANS = (2, 4, 8, 16)


def passed_along(shard, axis, by):
    size = lax.axis_size(axis)
    pairs = [(i, i + by) for i in range(size) if 0 <= i + by < size]
    return lax.ppermute(shard, axis, pairs)


def windowed_attend(
    query_rows, key_rows, value_rows, key_tail, value_tail, sinks, kv_heads, group, first_pos
):
    rows = query_rows.shape[0]
    blocks = rows // WINDOW
    width = key_rows.shape[1]
    ext_keys = jnp.concatenate([key_tail, key_rows], 0)
    ext_values = jnp.concatenate([value_tail, value_rows], 0)

    def banded(table):
        return jnp.concatenate(
            [
                table[:rows].reshape(blocks, WINDOW, width),
                table[WINDOW:].reshape(blocks, WINDOW, width),
            ],
            axis=1,
        )

    band_keys = banded(ext_keys).reshape(blocks, 2 * WINDOW, kv_heads, HEAD_SIZE)
    band_values = banded(ext_values).reshape(blocks, 2 * WINDOW, kv_heads, HEAD_SIZE)
    query_blocks = query_rows.reshape(blocks, WINDOW, kv_heads, group, HEAD_SIZE)
    scores = jnp.einsum(
        "bqkgd,bskd->bkgqs", query_blocks, band_keys, preferred_element_type=jnp.float32
    ) * HEAD_SIZE ** (-0.5)
    query_pos = first_pos + jnp.arange(rows).reshape(blocks, WINDOW, 1)
    key_pos = (
        first_pos
        - WINDOW
        + jnp.arange(blocks).reshape(blocks, 1, 1) * WINDOW
        + jnp.arange(2 * WINDOW).reshape(1, 1, 2 * WINDOW)
    )
    offset = query_pos - key_pos
    allowed = (offset >= 0) & (offset < WINDOW) & (key_pos >= 0)
    scores = jnp.where(allowed[:, None, None], scores, -jnp.inf)
    sink_grid = sinks.reshape(1, kv_heads, group, 1, 1)
    top = jnp.maximum(jnp.max(scores, axis=-1, keepdims=True), sink_grid)
    weights = jnp.exp(scores - top)
    total = jnp.sum(weights, axis=-1, keepdims=True) + jnp.exp(sink_grid - top)
    probs = (weights / total).astype(jnp.bfloat16)
    mixed = jnp.einsum(
        "bkgqs,bskd->bqkgd", probs, band_values, preferred_element_type=jnp.float32
    ).astype(jnp.bfloat16)
    row_log_weight_sum = (top + jnp.log(total))[..., 0]
    return (
        mixed.reshape(rows, kv_heads * group * HEAD_SIZE),
        row_log_weight_sum.transpose(1, 2, 0, 3).reshape(kv_heads * group, rows),
    )


def pool_branch(pool_rows, pool_tail, mixing, scales, group_start, first_pos):
    rows = pool_rows.shape[0]
    columns = pool_rows.shape[1]
    pool_reach = max(POOL_SPANS)
    extended = jnp.concatenate([pool_tail, pool_rows], 0).astype(jnp.float32)
    group_index = group_start + jnp.arange(columns) // POOL_CH
    span_table = jnp.array(POOL_SPANS, jnp.int32)
    matches = group_index[:, None] == jnp.arange(len(POOL_SPANS))[None, :]
    span_of_col = jnp.sum(jnp.where(matches, span_table[None, :], 0), axis=1)
    trailing = jnp.zeros((rows, columns), jnp.float32)
    for lag in range(pool_reach):
        trailing = trailing + jnp.where(
            lag < span_of_col[None, :], extended[pool_reach - lag : pool_reach - lag + rows], 0.0
        )
    position = first_pos + jnp.arange(rows)
    count = jnp.minimum(position[:, None] + 1, span_of_col[None, :]).astype(jnp.float32)
    centred = (trailing / count - extended[pool_reach:]).astype(jnp.bfloat16)
    grouped = centred.reshape(rows, columns // POOL_CH, POOL_CH)
    product = jnp.einsum(
        "rgc,gcd->rgd", grouped, mixing, preferred_element_type=jnp.float32
    ).reshape(rows, columns)
    return (product * scales).astype(jnp.bfloat16)


def local(
    tokens,
    norm_gain,
    query_weight,
    key_matrix,
    value_matrix,
    pool_in_weight,
    head_sink_logit,
    pool_mix,
    pool_gain,
    attn_out_weight,
    pool_out_weight,
):
    tp_index = lax.axis_index("tp")
    sp_index = lax.axis_index("sp")
    q_cols = query_weight.shape[1]
    kv_cols = key_matrix.shape[1]
    pool_cols = pool_in_weight.shape[1]
    q_heads = q_cols // HEAD_SIZE
    kv_heads = kv_cols // HEAD_SIZE
    groups_dev = pool_cols // POOL_CH
    full_query, full_key, full_value, full_pool = (
        lax.all_gather(query_weight, "sp", axis=0, tiled=True),
        lax.all_gather(key_matrix, "sp", axis=0, tiled=True),
        lax.all_gather(value_matrix, "sp", axis=0, tiled=True),
        lax.all_gather(pool_in_weight, "sp", axis=0, tiled=True),
    )
    values_f = lax.all_gather(tokens[0], "tp", axis=0, tiled=True).astype(jnp.float32)
    scale = lax.rsqrt(jnp.mean(values_f * values_f, axis=-1, keepdims=True) + EPSILON)
    normed = (values_f * scale * norm_gain).astype(jnp.bfloat16)
    outputs = [
        jnp.dot(normed, weight, preferred_element_type=jnp.float32).astype(jnp.bfloat16)
        for weight in (full_query, full_key, full_value, full_pool)
    ]
    projected = jnp.concatenate(outputs, axis=1)
    rows = projected.shape[0]
    first_pos = sp_index * rows
    query_rows = projected[:, :q_cols]
    key_rows = projected[:, q_cols : q_cols + kv_cols]
    value_rows = projected[:, q_cols + kv_cols : q_cols + 2 * kv_cols]
    pool_rows = projected[:, q_cols + 2 * kv_cols :]
    pool_reach = max(POOL_SPANS)
    sinks = lax.dynamic_slice_in_dim(head_sink_logit, tp_index * q_heads, q_heads, 0)
    mixing = lax.dynamic_slice_in_dim(pool_mix, tp_index * groups_dev, groups_dev, 0)
    scales = lax.dynamic_slice_in_dim(pool_gain, tp_index * pool_cols, pool_cols, 0)
    key_tail, value_tail, pool_tail = passed_along(
        (key_rows[rows - WINDOW :], value_rows[rows - WINDOW :], pool_rows[rows - pool_reach :]),
        "sp",
        1,
    )
    attn_part, log_part = windowed_attend(
        query_rows,
        key_rows,
        value_rows,
        key_tail,
        value_tail,
        sinks,
        kv_heads,
        q_heads // kv_heads,
        first_pos,
    )
    pool_part = pool_branch(pool_rows, pool_tail, mixing, scales, tp_index * groups_dev, first_pos)
    half_attn, half_pool = (
        lax.all_gather(attn_out_weight, "sp", axis=1, tiled=True),
        lax.all_gather(pool_out_weight, "sp", axis=1, tiled=True),
    )
    result = lax.psum_scatter(
        jnp.dot(attn_part, half_attn, preferred_element_type=jnp.float32)
        + jnp.dot(pool_part, half_pool, preferred_element_type=jnp.float32),
        "tp",
        scatter_dimension=0,
        tiled=True,
    ).astype(jnp.bfloat16)
    return (result[None], log_part[None])


LANES = 128
TILE = 16
OUT_CUTS = 4
MESH_ID = pl.DeviceIdType.MESH


def nearest(n, step, me):
    tables = [sorted((j for j in range(n) if j != z), key=lambda j: (abs(j - z), j)) for z in range(n)]
    shard = jnp.int32(tables[0][step])
    for z in range(1, n):
        shard = jnp.where(me == z, tables[z][step], shard)
    return shard


def layer_kernel(
    n,
    sinks,
    tokens,
    gain,
    wq,
    wk,
    wv,
    wp,
    mix,
    pool_gain,
    wao,
    wpo,
    out,
    log_out,
    held,
    wout,
    kv_in,
    tok,
    gain_v,
    pgain_v,
    sink_v,
    out_v,
    log_v,
    acc_q,
    acc_p,
    nrm,
    qb,
    kvb,
    pool_ext,
    mixed,
    mix_own,
    logs,
    logs_got,
    keep_n,
    send_n,
    got_n,
    y_part,
    y_got,
    keep_m,
    send_m,
    got_m,
    y_part_m,
    y_got_m,
    mine,
    sent,
    got,
    z_send,
    x_send,
    z_recv,
    x_recv,
    load_sem,
    tok_sem,
    tok_send,
    tok_recv,
    ytok_send,
    ytok_recv,
    fwd_send,
    fwd_recv,
    halo_send,
    halo_recv,
    sumn_send,
    sumn_recv,
    sumo_send,
    sumo_recv,
    yp_send,
    yp_recv,
    log_send,
    log_recv,
    out_sem,
):
    me = lax.axis_index("sp")
    f = lax.axis_index("fs")
    c = lax.axis_index("tp")
    f32, bf16 = jnp.float32, jnp.bfloat16
    half, width = tokens.shape
    rows = 2 * half
    depth = wq.shape[0]
    part_rows = depth // 2
    q_cols = wq.shape[1] // 2
    group = q_cols // HEAD_SIZE
    out_cols = wao.shape[1]
    n_in = held.shape[1] + 1
    n_pieces = n_in + OUT_CUTS
    n_units = n_pieces - 1
    chunk = half // 4
    blocks = rows // WINDOW
    y, x = f // 2, lax.rem(f, 2)
    beside = f + 1 - 2 * x
    across = lax.rem(f + 2, 4)
    up, down = me + 1, me - 1
    has_up, has_down = me < n - 1, me > 0
    inner = has_up & has_down

    def at_cols(ref, i):
        return ref.at[:, pl.ds(pl.multiple_of(y * q_cols + i * LANES, LANES), LANES)]

    y_rows = pl.ds(pl.multiple_of(y * part_rows, part_rows), part_rows)
    pool_index = 2 * c + y
    norm_order = (2, 0, 1, 3)

    def own_chunk(i, side):
        first = (3, 1, 2, 0) if side == 0 else (0, 2, 1, 3)
        return first[i] * chunk

    def own_at(i):
        return pl.multiple_of(jnp.where(c == 0, own_chunk(i, 0), own_chunk(i, 1)), chunk)

    def tok_load(i):
        at = pl.ds(own_at(i), chunk)
        return pltpu.make_async_copy(tokens.at[at], tok.at[at], tok_sem.at[i])

    first_loads = [
        pltpu.make_async_copy(wk, kv_in.at[0], load_sem.at[0]),
        pltpu.make_async_copy(wv, kv_in.at[1], load_sem.at[0]),
    ]
    for i in range(2):
        first_loads.append(pltpu.make_async_copy(at_cols(wq, i), held.at[me, 1 + i], load_sem.at[0]))
    for i in range(2):
        first_loads.append(pltpu.make_async_copy(at_cols(wp, i), held.at[me, 3 + i], load_sem.at[0]))
    out_loads = []
    for i in range(out_cols // LANES):
        for side, w in enumerate((wao, wpo)):
            to = wout.at[me, i, pl.ds(side * part_rows, part_rows)]
            out_loads.append(pltpu.make_async_copy(w.at[y_rows, pl.ds(i * LANES, LANES)], to, load_sem.at[1]))
    late_loads = [
        pltpu.make_async_copy(mix.at[pool_index], mix_own, load_sem.at[3]),
        pltpu.make_async_copy(pool_gain, pgain_v, load_sem.at[4]),
        pltpu.make_async_copy(sinks, sink_v, load_sem.at[5]),
    ]
    gain_load = pltpu.make_async_copy(gain, gain_v, load_sem.at[6])
    barrier = pltpu.get_barrier_semaphore()
    for peer in ({"tp": 1 - c}, {"fs": beside}, {"fs": across}, {"fs": across, "tp": 1 - c}):
        pl.semaphore_signal(barrier, inc=1, device_id=peer, device_id_type=MESH_ID)

    @pl.when(has_up)
    def _():
        pl.semaphore_signal(barrier, inc=1, device_id={"sp": up}, device_id_type=MESH_ID)

    @pl.when(has_down)
    def _():
        pl.semaphore_signal(barrier, inc=1, device_id={"sp": down}, device_id_type=MESH_ID)

    for cp in first_loads[:2]:
        cp.start()
    tok_load(norm_order[0]).start()
    gain_load.start()
    for cp in first_loads[2:]:
        cp.start()
    for i in norm_order[1:]:
        tok_load(i).start()
    for cp in out_loads + late_loads:
        cp.start()

    def remote(src, dst, send, recv, to):
        return pltpu.make_async_remote_copy(src, dst, send, recv, device_id=to, device_id_type=MESH_ID)

    def piece(s, j, part):
        if s < n_in - 2:
            return held.at[j, s, pl.ds(pl.multiple_of(part * part_rows, part_rows), part_rows)]
        if s < n_in:
            size = part_rows // 2
            return held.at[j, n_in - 2, pl.ds(pl.multiple_of(part * part_rows + (s - n_in + 2) * size, size), size)]
        block, side = divmod(s - n_in, 2)
        return wout.at[j, 2 * part + block, pl.ds(side * part_rows, part_rows)]

    def bulk(count):
        return nrm.at[0, pl.ds(0, count * part_rows * LANES // width)]

    def sent_all(ref, sem):
        pltpu.make_async_remote_copy(ref, ref, sem, sem, device_id={"tp": 1 - c}, device_id_type=MESH_ID).wait_send()

    def got_all(ref, sem):
        pltpu.make_async_remote_copy(ref, ref, sem, sem, device_id={"tp": 1 - c}, device_id_type=MESH_ID).wait_recv()

    def z_hop(s, j, way):
        block = piece(s, j, x)
        to = me if way is None else jnp.where(way == 0, up, down)
        slot = z_recv.at[s, lax.rem(j - to + n, n) - 1]
        return remote(block, block, z_send.at[0 if way is None else way], slot, {"sp": to})

    def x_group(s, k):
        if s >= n_in:
            return 5 + k
        return 0 if s == 0 else 1 + 2 * min((s - 1) // 2, 1) + k // (n - 2)

    def x_hop(s, k):
        block = piece(s, shard[k], x)
        return remote(block, block, x_send, x_recv.at[x_group(s, k)], {"fs": beside})

    def onward(j):
        return jnp.where(j < me, 0, 1), ((j < me) & has_up) | ((j > me) & has_down)

    def own_send(s):
        @pl.when(has_up)
        def _():
            z_hop(s, me, 0).start()

        @pl.when(has_down)
        def _():
            z_hop(s, me, 1).start()

    shard = [nearest(n, k, me) for k in range(n - 1)]
    def pass_on(s, k):
        j = shard[k]
        z_hop(s, j, None).wait_recv()
        way, more = onward(j)

        @pl.when(more)
        def _():
            z_hop(s, j, way).start()

        x_hop(s, k).start()

    def inner_slot(s, k):
        @pl.when(inner)
        def _():
            pass_on(s, k)

    def end_slot(s, k):
        @pl.when(jnp.logical_not(inner))
        def _():
            pass_on(s, k)

    def send_inner(s):
        @pl.when(inner)
        def _():
            own_send(s)

    def send_end(s):
        @pl.when(jnp.logical_not(inner))
        def _():
            own_send(s)

    def pick(a, b):
        return pl.ds(pl.multiple_of(jnp.where(c == 0, a, b), chunk), chunk)

    def tok_hop(i):
        block = nrm.at[0, pick(own_chunk(i, 0), half + own_chunk(i, 1))]
        return remote(block, block, tok_send, tok_recv, {"tp": 1 - c})

    low_order = (2, 4, 6, 0)
    high_order = (5, 3, 7, 1)

    def y_tok(i):
        where = pick(low_order[i] * chunk, high_order[i] * chunk)
        return remote(nrm.at[0, where], nrm.at[1, where], ytok_send, ytok_recv.at[i], {"fs": across})

    def fwd(i):
        block = nrm.at[1, pick(low_order[i] * chunk, high_order[i] * chunk)]
        return remote(block, block, fwd_send, fwd_recv.at[i], {"tp": 1 - c})

    @pl.when(me == 0)
    def _():
        for s in range(2):
            kvb[s, pl.ds(0, WINDOW), :] = jnp.zeros((WINDOW, kvb.shape[2]), bf16)
            pool_ext[s, pl.ds(0, TILE), :] = jnp.zeros((TILE, POOL_CH), bf16)

    first = nrm.at[0, pl.ds(0, len(first_loads) * depth * LANES // width)]
    pltpu.make_async_copy(first, first, load_sem.at[0]).wait()
    k_all, v_all = kv_in[0], kv_in[1]
    first = jnp.concatenate([k_all[:, :HEAD_SIZE], v_all[:, :HEAD_SIZE]], axis=1)
    second = jnp.concatenate([k_all[:, HEAD_SIZE:], v_all[:, HEAD_SIZE:]], axis=1)
    held[me, 0] = jnp.where(y == 0, first, second)
    gain_load.wait()
    pl.semaphore_wait(barrier, 4 + has_up.astype(jnp.int32) + has_down.astype(jnp.int32))
    strip = 32

    def norm(i):
        tok_load(i).wait()
        for part in range(chunk // strip):
            at = pl.multiple_of(own_at(i) + part * strip, strip)
            v = tok[pl.ds(at, strip), :].astype(f32)
            scale = lax.rsqrt(jnp.mean(v * v, axis=-1, keepdims=True) + EPSILON)
            nrm[0, pl.ds(pl.multiple_of(c * half + at, strip), strip), :] = (v * scale * gain_v[...]).astype(bf16)
        if i == norm_order[0]:
            y_tok(0).start()
        tok_hop(i).start()

    def own_tokens():
        got_all(nrm.at[0, pl.ds(0, half)], tok_recv)
        for i in range(1, 4):
            y_tok(i).start()

    def y_service(i):
        y_tok(i).wait_recv()
        fwd(i).start()

    def project(s, r0, size, cols, shards, acc=None):
        for j in shards:
            w = held[j, cols[0]] if len(cols) == 1 else jnp.concatenate([held[j, b] for b in cols], axis=1)
            deep = slice(j * depth, (j + 1) * depth) if isinstance(j, int) else pl.ds(pl.multiple_of(j * depth, depth), depth)
            term = jnp.dot(nrm[s, r0 : r0 + size, deep], w, preferred_element_type=f32)
            acc = term if acc is None else acc + term
        return acc

    every = range(n)
    early, last = [me] + shard[:-1], shard[-1:]

    def halo_kv(s):
        return remote(
            kvb.at[s, pl.ds(rows, WINDOW)], kvb.at[s, pl.ds(0, WINDOW)], halo_send.at[s], halo_recv.at[s], {"sp": up}
        )

    def halo_pool(s):
        return remote(
            pool_ext.at[s, pl.ds(rows, TILE)],
            pool_ext.at[s, pl.ds(0, TILE)],
            halo_send.at[2 + s],
            halo_recv.at[2 + s],
            {"sp": up},
        )

    def send_halo(halo, s):
        @pl.when(has_up)
        def _():
            halo(s).start()

    def wait_halo(halo, s):
        @pl.when(has_down)
        def _():
            halo(s).wait_recv()

    def project_kv(s, r0, size):
        kvb[s, pl.ds(WINDOW + r0, size), :] = project(s, r0, size, [0], every).astype(bf16)

    def project_q(s, r0, size):
        qb[s, pl.ds(r0, size), :] = project(s, r0, size, [1, 2], every).astype(bf16)

    def begin_q(s, r0, size):
        acc_q[s, pl.ds(r0, size), :] = project(s, r0, size, [1, 2], early)

    def end_q(s, r0, size):
        qb[s, pl.ds(r0, size), :] = project(s, r0, size, [1, 2], last, acc_q[s, pl.ds(r0, size), :]).astype(bf16)

    def project_pool(s, r0, size):
        pool_ext[s, pl.ds(TILE + r0, size), :] = project(s, r0, size, [3, 4], every).astype(bf16)

    def begin_pool(s, r0, size):
        acc_p[s, pl.ds(r0, size), :] = project(s, r0, size, [3, 4], early)

    def end_pool(s, r0, size):
        done = project(s, r0, size, [3, 4], last, acc_p[s, pl.ds(r0, size), :])
        pool_ext[s, pl.ds(TILE + r0, size), :] = done.astype(bf16)

    def attend(s, b):
        base = b * WINDOW
        lane = lax.broadcasted_iota(jnp.int32, (WINDOW, LANES), 1)
        lgs = jnp.zeros((WINDOW, LANES), f32)
        i_pos = lax.broadcasted_iota(jnp.int32, (WINDOW, 2 * WINDOW), 0)
        k_pos = lax.broadcasted_iota(jnp.int32, (WINDOW, 2 * WINDOW), 1)
        allowed = (k_pos > i_pos) & (k_pos <= i_pos + WINDOW)
        if b == 0:
            allowed = allowed & (k_pos + (me * rows - WINDOW) >= 0)
        band = kvb[s, pl.ds(base, 2 * WINDOW), :]
        keys, vals = band[:, :HEAD_SIZE], band[:, HEAD_SIZE:]
        q = qb[s, pl.ds(base, WINDOW), :]
        q = jnp.concatenate([q[:, h * HEAD_SIZE : (h + 1) * HEAD_SIZE] for h in range(group)], axis=0)
        scores = lax.dot_general(q, keys, (((1,), (1,)), ((), ())), preferred_element_type=f32)
        probs = []
        for h in range(group):
            sink = sink_v[(2 * c + y) * group + h]
            sc = jnp.where(allowed, scores[h * WINDOW : (h + 1) * WINDOW] * HEAD_SIZE**-0.5, -jnp.inf)
            top = jnp.maximum(jnp.max(sc, axis=-1, keepdims=True), sink)
            w = jnp.exp(sc - top)
            total = jnp.sum(w, axis=-1, keepdims=True) + jnp.exp(sink - top)
            probs.append((w * (1.0 / total)).astype(bf16))
            lgs = jnp.where(lane == h, top + jnp.log(total), lgs)
        res = jnp.dot(jnp.concatenate(probs, axis=0), vals, preferred_element_type=f32)
        res = jnp.concatenate([res[h * WINDOW : (h + 1) * WINDOW] for h in range(group)], axis=1)
        mixed[s, pl.ds(base, WINDOW), pl.ds(0, q_cols)] = res.astype(bf16)
        logs[s, :, pl.ds(base, WINDOW)] = jnp.transpose(lgs)[: logs.shape[1]]

    def pool(s, part):
        base = part * half
        run = pool_ext[s, pl.ds(base, TILE + half), :].astype(f32)
        own = run[TILE:]
        trailing = jnp.zeros_like(run)
        span_here = jnp.int32(0)
        reach = 1
        for at, span in enumerate(POOL_SPANS):
            while reach < span:
                run = run + pltpu.roll(run, reach, 0)
                reach *= 2
            trailing = jnp.where(pool_index == at, run, trailing)
            span_here = jnp.where(pool_index == at, span, span_here)
        pos = me * rows + base + lax.broadcasted_iota(jnp.int32, (half, 1), 0)
        count = jnp.minimum(pos + 1, span_here).astype(f32)
        centred = (trailing[TILE:] / count - own).astype(bf16)
        product = jnp.dot(centred, mix_own[...], preferred_element_type=f32)
        mixed[s, pl.ds(base, half), pl.ds(q_cols, POOL_CH)] = (product * pgain_v[pool_index]).astype(bf16)

    def log_hop():
        return remote(logs.at[1], logs_got, log_send, log_recv, {"fs": across})

    order = [me] + shard

    def unit(part, i, g):
        return part if i == 0 else 4 * (i - 1) + 2 * g + part

    def sum_n(part, i, g):
        u = unit(part, i, g)
        a, b = (send_n, got_n) if i == 0 else (send_m, got_m)
        return remote(a.at[u], b.at[u], sumn_send.at[min(i, 1)], sumn_recv.at[u + 2 * min(i, 1)], {"tp": 1 - c})

    def all_cols(j):
        return jnp.concatenate([wout[j, i] for i in range(out_cols // LANES)], axis=1)

    def sum_o(i):
        return remote(sent.at[i], got.at[i], sumo_send, sumo_recv.at[i], {"tp": 1 - c})

    def y_sum(part, i, g):
        u = unit(part, i, g)
        src, dst = (y_part.at[u], y_got.at[c]) if i == 0 else (y_part_m.at[u], y_got_m.at[i - 1, g, c])
        return remote(src, dst, yp_send.at[min(i, 1)], yp_recv.at[i], {"fs": across, "tp": part})

    def out_far(part, i, g):
        u = unit(part, i, g)
        j = order[i]
        keep, send = (keep_n, send_n) if i == 0 else (keep_m, send_m)
        if i == 0:
            w = all_cols(j)
        else:
            first = 2 * (x if g == 0 else 1 - x)
            w = jnp.concatenate([wout[j, first], wout[j, first + 1]], axis=1)
        acc = jnp.dot(mixed[1, part * half : (part + 1) * half, :], w, preferred_element_type=f32)
        across_cols = acc.shape[1] // 2
        left, right = acc[:, :across_cols], acc[:, across_cols:]
        keep[u] = jnp.where(c == 0, left, right)
        send[u] = jnp.where(c == 0, right, left).astype(bf16)
        sum_n(part, i, g).start()

    def pass_far(part, i, g):
        u = unit(part, i, g)
        keep, there, to = (keep_n, got_n, y_part) if i == 0 else (keep_m, got_m, y_part_m)
        sum_n(part, i, g).wait_recv()
        to[u] = (keep[u] + there[u].astype(f32)).astype(bf16)
        y_sum(part, i, g).start()

    def out_own(i):
        acc = jnp.dot(mixed[0], all_cols(order[i]), preferred_element_type=f32)
        low, high = acc[:half], acc[half:]
        mine[i] = jnp.where(c == 0, low, high)
        sent[i] = jnp.where(c == 0, high, low).astype(bf16)
        sum_o(i).start()

    def finish(i):
        sum_o(i).wait_recv()
        if i == 0:
            got_all(y_got, yp_recv.at[i])
            there = jnp.concatenate([y_got[0], y_got[1]], axis=1).astype(f32)
        else:
            got_all(y_got_m.at[i - 1], yp_recv.at[i])
            near = [y_got_m[i - 1, 0, 0], y_got_m[i - 1, 0, 1]]
            other = [y_got_m[i - 1, 1, 0], y_got_m[i - 1, 1, 1]]
            there = jnp.where(
                x == 0, jnp.concatenate(near + other, axis=1), jnp.concatenate(other + near, axis=1)
            ).astype(f32)
        out_v[i] = (mine[i] + got[i].astype(f32) + there).astype(bf16)
        out_copy(i).start()

    def out_copy(i):
        cols = pl.ds(pl.multiple_of(order[i] * out_cols, out_cols), out_cols)
        return pltpu.make_async_copy(out_v.at[i], out.at[:, cols], out_sem.at[0])

    log_copy = pltpu.make_async_copy(log_v, log_out, out_sem.at[1])

    def send_log():
        log_hop().start()

    def write_log():
        log_hop().wait()
        own_logs, far_logs = logs[0, :group], logs_got[:group]
        log_v[...] = jnp.where(
            y == 0, jnp.concatenate([own_logs, far_logs], axis=0), jnp.concatenate([far_logs, own_logs], axis=0)
        )
        log_copy.start()

    def drain():
        for z in range(n):

            @pl.when(me == z)
            def _():
                if z < n - 1:
                    sent_all(bulk(n_units * (z + 1)), z_send.at[0])
                if z:
                    sent_all(bulk(n_units * (n - z)), z_send.at[1])

        sent_all(bulk(n_units * (n - 1)), x_send)
        for sem in (tok_send, ytok_send, fwd_send):
            sent_all(nrm.at[0, pl.ds(0, half)], sem)

        @pl.when(has_up)
        def _():
            for s in range(2):
                halo_kv(s).wait_send()
                halo_pool(s).wait_send()

    def ready(pieces, ks):
        got_all(bulk(len(pieces) * len(ks)), x_recv.at[x_group(pieces[0], ks[0])])

    def ready_out(k):
        got_all(bulk(OUT_CUTS), x_recv.at[x_group(n_in, k)])

    def arrived(i):
        fwd(i).wait_recv()

    def late_wait():
        pltpu.make_async_copy(wout.at[me], wout.at[me], load_sem.at[1]).wait()
        for cp in late_loads:
            cp.wait()

    W = WINDOW
    send_end(1)
    send_end(2)
    send_inner(1)
    norm(2)
    norm(0)
    norm(1)
    norm(3)
    send_inner(2)
    send_inner(0)
    send_end(0)
    end_slot(1, 0)
    end_slot(2, 0)
    inner_slot(1, 0)
    inner_slot(1, 1)
    own_tokens()
    end_slot(0, 0)
    inner_slot(2, 1)
    inner_slot(2, 0)
    end_slot(1, 1)
    inner_slot(0, 1)
    inner_slot(0, 0)
    send_end(3)
    inner_slot(1, 2)
    end_slot(2, 1)
    inner_slot(2, 2)
    late_wait()
    send_end(8)
    inner_slot(0, 2)
    send_end(4)
    send_inner(4)
    send_end(5)
    send_inner(5)
    end_slot(0, 1)
    send_inner(3)
    end_slot(1, 2)
    end_slot(2, 2)
    ready([1, 2], range(n - 2))
    begin_q(0, half, half)
    inner_slot(4, 1)
    inner_slot(4, 0)
    end_slot(0, 2)
    inner_slot(5, 1)
    send_end(6)
    end_slot(4, 0)
    inner_slot(5, 0)
    inner_slot(3, 0)
    end_slot(5, 0)
    inner_slot(3, 1)
    inner_slot(4, 2)
    begin_q(0, 0, half)
    ready([1, 2], [n - 2])
    end_q(0, 0, half)
    y_service(0)
    send_end(9)
    end_slot(3, 0)
    inner_slot(5, 2)
    end_q(0, half, half)
    ready([0], range(n - 1))
    project_kv(0, 0, half)
    inner_slot(3, 2)
    send_inner(6)
    end_slot(4, 1)
    y_service(1)
    end_slot(5, 1)
    attend(0, 1)
    y_service(2)
    project_kv(0, half, half)
    end_slot(3, 1)
    attend(0, 3)
    send_inner(8)
    send_inner(9)
    end_slot(4, 2)
    attend(0, 2)
    end_slot(5, 2)
    send_inner(7)
    arrived(0)
    arrived(1)
    begin_q(1, W, 2 * W)
    arrived(2)
    project_kv(1, 3 * W, W)
    send_halo(halo_kv, 1)
    send_end(7)
    end_slot(3, 2)
    inner_slot(6, 0)
    inner_slot(6, 1)
    end_q(1, W, 2 * W)
    project_kv(1, W, 2 * W)
    attend(1, 2)
    y_service(3)
    end_slot(6, 0)
    begin_q(1, 3 * W, W)
    end_q(1, 3 * W, W)
    attend(1, 3)
    ready([3, 4], range(n - 2))
    begin_pool(1, half - TILE, half + TILE)
    ready([3, 4], [n - 2])
    end_pool(1, half - TILE, half + TILE)
    pool(1, 1)
    out_far(1, 0, 0)
    end_slot(8, 0)
    send_halo(halo_pool, 1)
    inner_slot(7, 0)
    end_slot(9, 0)
    arrived(3)
    project_kv(1, 0, W)
    attend(1, 1)
    inner_slot(8, 0)
    inner_slot(9, 0)
    end_slot(7, 0)
    out_far(1, 1, 0)
    inner_slot(7, 1)
    inner_slot(8, 1)
    project_pool(1, 0, half - TILE)
    project_q(1, 0, W)
    pass_far(1, 0, 0)
    inner_slot(9, 1)
    wait_halo(halo_kv, 1)
    attend(1, 0)
    wait_halo(halo_pool, 1)
    pool(1, 0)
    out_far(0, 0, 0)
    end_slot(6, 1)
    pass_far(1, 1, 0)
    out_far(0, 1, 0)
    begin_pool(0, half, half)
    end_pool(0, half, half)
    send_halo(halo_pool, 0)
    send_halo(halo_kv, 0)
    inner_slot(7, 2)
    inner_slot(6, 2)
    end_slot(7, 1)
    begin_pool(0, 0, half)
    end_pool(0, 0, half)
    pool(0, 1)
    ready_out(0)
    out_far(0, 1, 1)
    out_far(1, 1, 1)
    pass_far(0, 0, 0)
    inner_slot(8, 2)
    pass_far(0, 1, 0)
    end_slot(8, 1)
    end_slot(9, 1)
    out_far(1, 2, 0)
    wait_halo(halo_pool, 0)
    pool(0, 0)
    out_far(0, 2, 0)
    inner_slot(9, 2)
    wait_halo(halo_kv, 0)
    attend(0, 0)
    out_own(0)
    pass_far(1, 1, 1)
    pass_far(0, 1, 1)
    end_slot(7, 2)
    out_own(1)
    pass_far(1, 2, 0)
    pass_far(0, 2, 0)
    end_slot(6, 2)
    ready_out(1)
    out_far(1, 2, 1)
    out_far(0, 2, 1)
    out_own(2)
    end_slot(8, 2)
    finish(0)
    end_slot(9, 2)
    out_far(1, 3, 0)
    out_far(0, 3, 0)
    pass_far(1, 2, 1)
    pass_far(0, 2, 1)
    finish(1)
    drain()
    pass_far(1, 3, 0)
    send_log()
    pass_far(0, 3, 0)
    ready_out(2)
    out_far(1, 3, 1)
    out_far(0, 3, 1)
    out_own(3)
    pass_far(1, 3, 1)
    pass_far(0, 3, 1)
    finish(2)
    write_log()
    finish(3)
    sent_all(send_n, sumn_send.at[0])
    sent_all(send_m, sumn_send.at[1])
    sent_all(sent, sumo_send)
    sent_all(y_part, yp_send.at[0])
    sent_all(y_part_m, yp_send.at[1])
    pltpu.make_async_copy(out, out, out_sem.at[0]).wait()
    log_copy.wait()


def fused_local(
    n,
    tokens,
    norm_gain,
    query_weight,
    key_matrix,
    value_matrix,
    pool_in_weight,
    head_sink_logit,
    pool_mix,
    pool_gain,
    attn_out_weight,
    pool_out_weight,
):
    _, half, width = tokens.shape
    rows = 2 * half
    depth, q_all = query_weight.shape
    heads = q_all // HEAD_SIZE
    kv_cols = key_matrix.shape[1]
    q_cols = q_all // 2
    out_cols = attn_out_weight.shape[1]
    n_in = 1 + 2 * (q_cols // LANES)
    pieces = n_in + 1 + OUT_CUTS
    bf16, f32 = jnp.bfloat16, jnp.float32
    dma = pltpu.SemaphoreType.DMA
    hbm = pl.BlockSpec(memory_space=pl.ANY)
    mixed, logs = pl.pallas_call(
        functools.partial(layer_kernel, n),
        out_shape=(
            jax.ShapeDtypeStruct((half, width), bf16),
            jax.ShapeDtypeStruct((heads, rows), f32),
        ),
        in_specs=[hbm] * 11,
        out_specs=(hbm, hbm),
        scratch_shapes=[
            pltpu.VMEM((n, n_in, depth, LANES), bf16),
            pltpu.VMEM((n, out_cols // LANES, depth, LANES), bf16),
            pltpu.VMEM((2, depth, kv_cols), bf16),
            pltpu.VMEM((half, width), bf16),
            pltpu.VMEM((1, width), f32),
            pltpu.VMEM((2 * 2, 1, POOL_CH), f32),
            pltpu.SMEM(head_sink_logit.shape, f32),
            pltpu.VMEM((n, half, out_cols), bf16),
            pltpu.VMEM((heads, rows), f32),
            pltpu.VMEM((2, rows, q_cols), f32),
            pltpu.VMEM((2, rows, POOL_CH), f32),
            pltpu.VMEM((2, rows, width), bf16),
            pltpu.VMEM((2, rows, q_cols), bf16),
            pltpu.VMEM((2, WINDOW + rows, kv_cols), bf16),
            pltpu.VMEM((2, TILE + rows, POOL_CH), bf16),
            pltpu.VMEM((2, rows, q_cols + POOL_CH), bf16),
            pltpu.VMEM((POOL_CH, POOL_CH), bf16),
            pltpu.VMEM((2, heads, rows), f32),
            pltpu.VMEM((heads, rows), f32),
            pltpu.VMEM((2, half, out_cols // 2), f32),
            pltpu.VMEM((2, half, out_cols // 2), bf16),
            pltpu.VMEM((2, half, out_cols // 2), bf16),
            pltpu.VMEM((2, half, out_cols // 2), bf16),
            pltpu.VMEM((2, half, out_cols // 2), bf16),
            pltpu.VMEM((4 * (n - 1), half, out_cols // 4), f32),
            pltpu.VMEM((4 * (n - 1), half, out_cols // 4), bf16),
            pltpu.VMEM((4 * (n - 1), half, out_cols // 4), bf16),
            pltpu.VMEM((4 * (n - 1), half, out_cols // 4), bf16),
            pltpu.VMEM((n - 1, 2, 2, half, out_cols // 4), bf16),
            pltpu.VMEM((n, half, out_cols), f32),
            pltpu.VMEM((n, half, out_cols), bf16),
            pltpu.VMEM((n, half, out_cols), bf16),
            dma((2,)),
            dma,
            dma((pieces, n - 1)),
            dma((5 + n - 1,)),
            dma((7,)),
            dma((4,)),
            dma,
            dma,
            dma,
            dma((4,)),
            dma,
            dma((4,)),
            dma((4,)),
            dma((4,)),
            dma((2,)),
            dma((2 + 4 * (n - 1),)),
            dma,
            dma((n,)),
            dma((2,)),
            dma((n,)),
            dma,
            dma,
            dma((2,)),
        ],
        compiler_params=pltpu.CompilerParams(
            collective_id=0, has_side_effects=True, vmem_limit_bytes=60 * 1024 * 1024
        ),
    )(
        head_sink_logit,
        tokens[0],
        norm_gain.reshape(1, width),
        query_weight,
        key_matrix,
        value_matrix,
        pool_in_weight,
        pool_mix,
        pool_gain.reshape(-1, 1, POOL_CH),
        attn_out_weight,
        pool_out_weight,
    )
    return mixed[None], logs[None]


def fits(mesh, tokens, query_weight, key_matrix, pool_in_weight, attn_out_weight):
    n, f, c = mesh.shape["sp"], mesh.shape["fs"], mesh.shape["tp"]
    depth = query_weight.shape[0] // n
    rows = tokens.shape[1] // n
    q_cols, kv_cols, pool_cols = (w.shape[1] // c for w in (query_weight, key_matrix, pool_in_weight))
    return (
        n == 4
        and f == 4
        and c == 2
        and tokens.shape[0] == f
        and rows == 4 * WINDOW
        and kv_cols == LANES == 2 * HEAD_SIZE
        and q_cols == 4 * LANES
        and pool_cols == 2 * POOL_CH == q_cols
        and attn_out_weight.shape[1] == n * 4 * LANES
        and attn_out_weight.shape[0] // c == depth == q_cols
    )


def solution(mesh):
    in_specs = (
        P("fs", ("sp", "tp"), None),
        P(),
        P("sp", "tp"),
        P("sp", "tp"),
        P("sp", "tp"),
        P("sp", "tp"),
        P(),
        P(),
        P(),
        P("tp", "sp"),
        P("tp", "sp"),
    )
    out_specs = (P("fs", ("sp", "tp"), None), P("fs", "tp", "sp"))

    def step(*args):
        fused = fits(mesh, args[0], args[2], args[3], args[5], args[9])
        body = functools.partial(fused_local, mesh.shape["sp"]) if fused else local
        mapped = jax.shard_map(body, mesh=mesh, in_specs=in_specs, out_specs=out_specs, check_vma=False)
        return mapped(*args)

    return step
```
